256 devices in a mesh: sp: 32 (over z, x), tp: 8 (over y, core).
Axes of the slice: x: 4, y: 4, z: 8, core: 2. Of those that a mesh axis runs over, the one named last changes fastest.
Arguments:
- tokens: bfloat16 [16384, 2048], P(('sp', 'tp')), may hold values from -64 to 64
- query_weight: bfloat16 [2048, 2048], P(None, 'tp'), may hold values from -0.125 to 0.125
- key_weight: bfloat16 [2048, 2048], P(None, 'tp'), may hold values from -0.125 to 0.125
- value_weight: bfloat16 [2048, 2048], P(None, 'tp'), may hold values from -0.125 to 0.125
- gate_weight: bfloat16 [2048, 2048], P(None, 'tp'), may hold values from -0.125 to 0.125
- forget_weight: bfloat16 [2048, 16], replicated, may hold values from -0.125 to 0.125
- forget_bias: float32 [16], replicated, as said below
- out_weight: bfloat16 [2048, 2048], replicated, may hold values from -0.125 to 0.125
Outputs:
- mixed: bfloat16 [16384, 2048], P(('sp', 'tp'))
The draws below stay inside these ranges and needn't reach their ends.
Inputs may be any that keep to these rules, and one draw needn't show every extreme that they name: `forget_bias`: every head's forget bias is at least 4.
All inputs are finite; a program needn't handle non-finite values.
Results may differ from the reference program's by a relative error of at most 0.015.
The reference program's roundings to bfloat16 on the way (of `queries`, `keys`, `values` and `attended`) count: a program that leaves them out, or rounds other values in their place, can miss the bound.
Values may be sent and summed in bfloat16 or wider, within the bound.
No kernel may reach another device: no remote copies, remote signals or barrier semaphores. Data moves between devices by JAX's collectives and lax.ppermute only.
A program may use at most 128 MiB of HBM per device.

```python
import math
import jax
import jax.numpy as jnp
from jax import lax

D = 2048
HEADS = 16
HEAD_DIM = 128
TOK_DEV = 512
SEQ = 16384


def draw_tokens(key, part):
    keys = jax.random.split(jax.random.fold_in(key, 11), 5)
    span = max(TOK_DEV // 4, 1)
    blocks = SEQ // span
    base = jnp.clip(jax.random.normal(keys[0], (SEQ, D), jnp.float32), -4.0, 4.0)
    shifts = 0.7 * jnp.clip(jax.random.normal(keys[1], (blocks, D), jnp.float32), -2.0, 2.0)
    scales = jnp.exp(jax.random.uniform(keys[2], (blocks, 1), jnp.float32, jnp.log(0.5), jnp.log(2.0)))
    field = (base.reshape(blocks, span, D) + shifts[:, None, :]) * scales[:, None, :]
    field = field.reshape(SEQ, D)
    return jnp.clip(field, -64.0, 64.0).astype(jnp.bfloat16)


def draw_forget_bias(key, part):
    keys = jax.random.split(jax.random.fold_in(key, 23), 2)
    order = jax.random.permutation(keys[0], HEADS)
    fast_count = HEADS // 2
    fast = (order < fast_count).astype(jnp.float32)
    spread = jax.random.uniform(keys[1], (HEADS,), jnp.float32)
    slow_bias = jnp.log(jnp.float32(SEQ)) + 1.0 + spread
    fast_bias = 4.0 + 1.5 * spread
    return fast * fast_bias + (1.0 - fast) * slow_bias


def shard_levels(key, extent, shards, smallest, top_value):
    factor_of = 1.0
    for axis_at, shards_of in shards:
        steps = jax.random.uniform(jax.random.fold_in(jax.random.fold_in(key, 6), axis_at), (shards_of,), jnp.float32, smallest / len(shards), top_value / len(shards))
        factor_of = factor_of * jnp.repeat(jnp.exp(steps), extent[axis_at] // shards_of).reshape((-1,) + (1,) * (len(extent) - 1 - axis_at))
    return factor_of


def noise(stream_key, dims, width, bound, pieces=(), held_as=jnp.bfloat16):
    factor_of = shard_levels(stream_key, dims, pieces, -0.22, 0.18) if pieces else 1.0
    drawn = jax.random.normal(stream_key, dims, jnp.float32) * width * factor_of
    return jnp.minimum(jnp.maximum(drawn, -bound), bound).astype(held_as)


def setup_inputs(seed: int = 0) -> dict:
    streams_of = jax.random.split(jax.random.key(seed), 9)
    tokens = draw_tokens(jax.random.fold_in(streams_of[8], 71), 0)
    query_weight = noise(streams_of[1], (D, D), D ** -0.5, 0.125, ((1, 8),))
    key_weight = noise(streams_of[2], (D, D), D ** -0.5, 0.125, ((1, 8),))
    value_weight = noise(streams_of[3], (D, D), D ** -0.5, 0.125, ((1, 8),))
    gate_weight = noise(streams_of[4], (D, D), D ** -0.5, 0.125, ((1, 8),))
    forget_weight = noise(streams_of[5], (D, HEADS), D ** -0.5, 0.125)
    forget_bias = draw_forget_bias(jax.random.fold_in(streams_of[8], 71), 0)
    out_weight = noise(streams_of[7], (D, D), D ** -0.5, 0.125)
    return {"tokens": tokens, "query_weight": query_weight, "key_weight": key_weight, "value_weight": value_weight, "gate_weight": gate_weight, "forget_weight": forget_weight, "forget_bias": forget_bias, "out_weight": out_weight}


def reference(tokens, query_weight, key_weight, value_weight, gate_weight, forget_weight, forget_bias, out_weight):
    scale = HEAD_DIM ** -0.5
    queries = (jnp.dot(tokens, query_weight, preferred_element_type=jnp.float32) * scale).astype(jnp.bfloat16)
    keys = jnp.dot(tokens, key_weight, preferred_element_type=jnp.float32).astype(jnp.bfloat16)
    values = jnp.dot(tokens, value_weight, preferred_element_type=jnp.float32).astype(jnp.bfloat16)
    gate = jax.nn.sigmoid(jnp.dot(tokens, gate_weight, preferred_element_type=jnp.float32))
    forget_log = jax.nn.log_sigmoid(jnp.dot(tokens, forget_weight, preferred_element_type=jnp.float32) + forget_bias)
    cumul = jnp.cumsum(forget_log.T, axis=1)
    span = math.gcd(SEQ, 512)
    blocks = SEQ // span
    positions = jnp.arange(SEQ, dtype=jnp.int32)

    def one_head(args):
        head_q, head_k, head_v, head_c = args
        query_blocks = head_q.reshape(blocks, span, HEAD_DIM)
        cum_blocks = head_c.reshape(blocks, span)
        pos_blocks = positions.reshape(blocks, span)

        def one_block(inner):
            block_q, block_c, block_p = inner
            scores = jnp.dot(block_q, head_k.T, preferred_element_type=jnp.float32)
            scores = scores + block_c[:, None] - head_c[None, :]
            scores = jnp.where(positions[None, :] <= block_p[:, None], scores, -jnp.inf)
            top = jnp.max(scores, axis=1, keepdims=True)
            weights = jnp.exp(scores - top)
            denom = jnp.sum(weights, axis=1, keepdims=True)
            return jnp.dot(weights.astype(jnp.bfloat16), head_v, preferred_element_type=jnp.float32) / denom

        return lax.map(one_block, (query_blocks, cum_blocks, pos_blocks)).reshape(SEQ, HEAD_DIM)

    split_q = queries.reshape(SEQ, HEADS, HEAD_DIM).transpose(1, 0, 2)
    split_k = keys.reshape(SEQ, HEADS, HEAD_DIM).transpose(1, 0, 2)
    split_v = values.reshape(SEQ, HEADS, HEAD_DIM).transpose(1, 0, 2)
    heads_out = lax.map(one_head, (split_q, split_k, split_v, cumul))
    heads_out = heads_out.transpose(1, 0, 2).reshape(SEQ, D)
    attended = (heads_out * gate).astype(jnp.bfloat16)
    return jnp.dot(attended, out_weight, preferred_element_type=jnp.float32).astype(jnp.bfloat16)
```

```python
import functools

import jax
import jax.numpy as jnp
from jax import lax
from jax.experimental import pallas as pl
from jax.experimental.pallas import tpu as pltpu
from jax.sharding import Mesh
from jax.sharding import PartitionSpec as P

HEAD_DIM = 128
NZ, NX, NY, NC = 8, 4, 4, 2
BLOCK = 512
HALF = 256
SLAB = NX * BLOCK
PIECE = 64
WIDTH = 2048
COLS = 256
META = 16
NEG = -1e30

VMEM = pltpu.VMEM
SMEM = pltpu.SMEM
BF = jnp.bfloat16
F32 = jnp.float32


def vspec():
    return pl.BlockSpec(memory_space=VMEM)


def sspec():
    return pl.BlockSpec(memory_space=SMEM)


def thirds(value):
    high = value.astype(BF).astype(F32)
    rest = value - high
    mid = rest.astype(BF).astype(F32)
    low = (rest - mid).astype(BF).astype(F32)
    return high, mid, low


def key_kernel(pos_ref, *refs):
    pieces = refs[:8]
    wk_ref, fw_ref, bias_ref, toks_ref, kx_ref = refs[8:]
    for i in range(8):
        start = pl.multiple_of(pos_ref[i] * PIECE, PIECE)
        toks_ref[pl.ds(start, PIECE), :] = pieces[i][...]
    toks = toks_ref[...]
    keys = jnp.dot(toks, wk_ref[...], preferred_element_type=F32).astype(BF)
    logits = lax.dot_general(
        fw_ref[...], toks, (((1,), (1,)), ((), ())), preferred_element_type=F32
    )
    logits = logits + bias_ref[:, :1]
    logs = jnp.minimum(logits, 0.0) - jnp.log1p(jnp.exp(-jnp.abs(logits)))
    row = lax.broadcasted_iota(jnp.int32, (BLOCK, BLOCK), 0)
    col = lax.broadcasted_iota(jnp.int32, (BLOCK, BLOCK), 1)
    upper = (row <= col).astype(BF)
    local = sum(
        jnp.dot(part.astype(BF), upper, preferred_element_type=F32) for part in thirds(logs)
    )
    parts = thirds(local)
    whole = [jnp.broadcast_to(part[:, BLOCK - 1 :], (META, 128)) for part in parts]
    for b in range(2):
        for a in range(2):
            dest = 2 * b + a
            kx_ref[dest, :HALF, :] = keys[b * HALF : (b + 1) * HALF, a * 128 : (a + 1) * 128]
            rows = [
                part[a : a + 1, b * HALF + i * 128 : b * HALF + (i + 1) * 128]
                for part in parts
                for i in range(2)
            ]
            rows += [part[a : a + 1, :] for part in whole]
            rows.append(jnp.zeros((META - 9, 128), F32))
            kx_ref[dest, HALF:, :] = jnp.concatenate(rows, axis=0).astype(BF)


def value_kernel(toks_ref, wv_ref, vx_ref):
    values = jnp.dot(toks_ref[...], wv_ref[...], preferred_element_type=F32).astype(BF)
    for b in range(2):
        for a in range(2):
            vx_ref[2 * b + a] = values[b * HALF : (b + 1) * HALF, a * 128 : (a + 1) * 128]


def query_kernel(toks_ref, wq_ref, qx_ref):
    queries = jnp.dot(toks_ref[...], wq_ref[...], preferred_element_type=F32)
    queries = (queries * HEAD_DIM**-0.5).astype(BF)
    for b in range(2):
        for a in range(2):
            qx_ref[2 * b + a] = queries[:, a * 128 : (a + 1) * 128]


def gate_kernel(toks_ref, wg_ref, gate_ref):
    pre = jnp.dot(toks_ref[...], wg_ref[...], preferred_element_type=F32)
    gate = 1.0 / (1.0 + jnp.exp(-pre))
    for a in range(2):
        gate_ref[a] = gate[:, a * 128 : (a + 1) * 128]


QB = 512
QS = 256


def slab_bias(k_ref):
    biases = []
    before = jnp.zeros((1, 128), F32)
    for xs in range(NX):
        meta = k_ref[xs, HALF:, :].astype(F32)
        rows = [meta[i : i + 1] + meta[2 + i : 3 + i] + meta[4 + i : 5 + i] for i in range(2)]
        biases.append(jnp.concatenate([r + before for r in rows], axis=1))
        before = before + (meta[6:7] + meta[7:8] + meta[8:9])
    return biases, before


def attend(flag_ref, q_ref, k_ref, v_ref, base, biases, diag, state):
    for i in range(QB // QS):
        q = q_ref[i * QS : (i + 1) * QS, :]
        scores = []
        for xs in range(NX):
            s = lax.dot_general(
                q, k_ref[xs, :HALF, :], (((1,), (1,)), ((), ())), preferred_element_type=F32
            )
            s = s - (biases[xs] + base)
            if diag:
                first = pl.program_id(0) * QB + i * QS - xs * BLOCK - flag_ref[1] * HALF
                row = lax.broadcasted_iota(jnp.int32, (QS, HALF), 0)
                col = lax.broadcasted_iota(jnp.int32, (QS, HALF), 1)
                s = jnp.where(col - row <= first, s, NEG)
            scores.append(s)
        best = jnp.max(functools.reduce(jnp.maximum, scores), axis=1, keepdims=True)
        old = state(i)
        if old is not None:
            best = jnp.maximum(best, old[0])
        safe = jnp.where(best < -1e29, 0.0, best) if diag else best
        total = 0.0
        accum = 0.0
        for xs in range(NX):
            w = jnp.exp(scores[xs] - safe)
            total = total + jnp.sum(w, axis=1, keepdims=True)
            accum = accum + jnp.dot(w.astype(BF), v_ref[xs], preferred_element_type=F32)
        if old is not None:
            factor = jnp.exp(old[0] - safe)
            total = total + old[1] * factor
            accum = accum + old[2] * factor
        yield i, best, total, accum


def put_state(ml_ref, acc_ref, i, best, total, accum):
    lane = lax.broadcasted_iota(jnp.int32, (QS, 128), 1)
    ml_ref[i * QS : (i + 1) * QS, :] = jnp.where(lane < 64, best, total)
    acc_ref[i * QS : (i + 1) * QS, :] = accum


def get_state(ml_ref, acc_ref, i):
    ml = ml_ref[i * QS : (i + 1) * QS, :]
    return ml[:, :1], ml[:, 64:65], acc_ref[i * QS : (i + 1) * QS, :]


def first_kernel(diag, flag_ref, q_ref, k_ref, v_ref, off_out, ml_out, acc_out):
    biases, whole = slab_bias(k_ref)
    mode = flag_ref[0]

    @pl.when(mode == 1)
    def _():
        for args in attend(
            flag_ref, q_ref, k_ref, v_ref, 0.0, biases, diag, lambda i: None
        ):
            put_state(ml_out, acc_out, *args)
        off_out[...] = jnp.broadcast_to(jnp.zeros_like(whole) if diag else whole, (8, 128))

    @pl.when(mode == 0)
    def _():
        off_out[...] = jnp.zeros((8, 128), F32)
        lane = lax.broadcasted_iota(jnp.int32, (QB, 128), 1)
        ml_out[...] = jnp.where(lane < 64, NEG, 0.0)
        acc_out[...] = jnp.zeros((QB, 128), F32)


def next_kernel(
    forward, flag_ref, q_ref, k_ref, v_ref, off_in, ml_in, acc_in, off_out, ml_out, acc_out
):
    biases, whole = slab_bias(k_ref)
    mode = flag_ref[0]
    off = off_in[:1, :]
    base = off - whole if forward else off

    @pl.when(mode == 1)
    def _():
        base2 = jnp.concatenate([base, base], axis=1)
        for args in attend(
            flag_ref, q_ref, k_ref, v_ref, base2, biases, False,
            lambda i: get_state(ml_in, acc_in, i),
        ):
            put_state(ml_out, acc_out, *args)
        off_out[...] = jnp.broadcast_to(base if forward else off + whole, (8, 128))

    @pl.when(mode == 0)
    def _():
        off_out[...] = off_in[...]
        ml_out[...] = ml_in[...]
        acc_out[...] = acc_in[...]


def last_kernel(
    flag_ref, q_ref, k_ref, v_ref, foff, fml, facc, boff, bml, bacc, out_ref, ml_s, acc_s
):
    biases, whole = slab_bias(k_ref)
    mode = flag_ref[0]
    gain = (mode == 1).astype(F32)
    base = foff[:1, :] - whole * gain

    @pl.when(mode == 1)
    def _():
        base2 = jnp.concatenate([base, base], axis=1)
        for args in attend(
            flag_ref, q_ref, k_ref, v_ref, base2, biases, False,
            lambda i: get_state(fml, facc, i),
        ):
            put_state(ml_s, acc_s, *args)

    @pl.when(mode == 0)
    def _():
        ml_s[...] = fml[...]
        acc_s[...] = facc[...]

    shift = (boff[:1, :] - base)[:, :1]
    stats = []
    for i in range(QB // QS):
        best_f, total_f, acc_f = get_state(ml_s, acc_s, i)
        best_b, total_b, acc_b = get_state(bml, bacc, i)
        best_b = jnp.where(total_b > 0.0, best_b + shift, NEG)
        best = jnp.maximum(best_f, best_b)
        safe = jnp.where(best < -1e29, 0.0, best)
        wf = jnp.exp(best_f - safe)
        wb = jnp.exp(best_b - safe)
        total = wf * total_f + wb * total_b
        some = total > 0.0
        total = jnp.where(some, total, 1.0)
        out = (wf * acc_f + wb * acc_b) / total
        out_ref[0, i * QS : (i + 1) * QS, :] = out.astype(BF)
        lse = jnp.broadcast_to(jnp.where(some, best + jnp.log(total), NEG), (QS, 128))
        for g in range(QS // 128):
            stats.append(lse[g * 128 : (g + 1) * 128, :].T[:1, :])
    stats = jnp.concatenate(stats, axis=0)
    rows = jnp.concatenate([*thirds(stats), jnp.zeros((META - 12, 128), F32)], axis=0)
    out_ref[0, BLOCK:, :] = rows.astype(BF)


def join_kernel(part_ref, gate_ref, out_ref):
    for a in range(2):
        lses = []
        for b in range(2):
            meta = part_ref[2 * b + a, BLOCK:, :].astype(F32)
            lses.append(meta[0:4] + meta[4:8] + meta[8:12])
        for g in range(4):
            rows = slice(g * 128, (g + 1) * 128)
            l0, l1 = [jnp.broadcast_to(lse[g : g + 1], (128, 128)).T for lse in lses]
            best = jnp.maximum(l0, l1)
            w0 = jnp.exp(l0 - best)
            w1 = jnp.exp(l1 - best)
            mix = w0 * part_ref[a, rows, :].astype(F32) + w1 * part_ref[2 + a, rows, :].astype(F32)
            att = (mix / (w0 + w1) * gate_ref[a, rows, :]).astype(BF)
            for h in range(2):
                out_ref[2 * g + h, :, a * 128 : (a + 1) * 128] = att[h * PIECE : (h + 1) * PIECE]


def shape(*dims, dtype=BF):
    return jax.ShapeDtypeStruct(dims, dtype)


def cost(flops, bytes_accessed=4 << 20, exps=0):
    return pl.CostEstimate(flops=flops, bytes_accessed=bytes_accessed, transcendentals=exps)


def plain(kernel, outs, n_in, name, flops, smem=0, scratch=()):
    return pl.pallas_call(
        kernel,
        out_shape=outs,
        in_specs=[sspec()] * smem + [vspec()] * (n_in - smem),
        out_specs=jax.tree.map(lambda _: vspec(), outs),
        scratch_shapes=scratch,
        name=name,
        cost_estimate=cost(flops),
    )


STATE = (shape(8, 128, dtype=F32), shape(SLAB, 128, dtype=F32), shape(SLAB, 128, dtype=F32))
STATE_SPECS = [
    pl.BlockSpec((8, 128), lambda i: (0, 0)),
    pl.BlockSpec((QB, 128), lambda i: (i, 0)),
    pl.BlockSpec((QB, 128), lambda i: (i, 0)),
]
QKV_SPECS = [
    pl.BlockSpec((QB, 128), lambda i: (i, 0)),
    pl.BlockSpec((NX, HALF + META, 128), lambda i: (0, 0, 0)),
    pl.BlockSpec((NX, HALF, 128), lambda i: (0, 0, 0)),
]
ATT_FLOPS = 4 * SLAB * NX * HALF * 128


def attention_call(kind, diag=False, forward=True):
    if kind == "first":
        kernel, states = functools.partial(first_kernel, diag), 0
    elif kind == "next":
        kernel, states = functools.partial(next_kernel, forward), 1
    else:
        kernel, states = last_kernel, 2
    outs, out_specs, scratch, alias = STATE, STATE_SPECS, [], {}
    if kind == "next":
        alias = {4: 0, 5: 1, 6: 2}
    if kind == "last":
        outs = shape(NX, BLOCK + META, 128)
        out_specs = pl.BlockSpec((1, BLOCK + META, 128), lambda i: (i, 0, 0))
        scratch = [VMEM((QB, 128), F32), VMEM((QB, 128), F32)]
        alias = {}
    return pl.pallas_call(
        kernel,
        out_shape=outs,
        grid=(SLAB // QB,),
        in_specs=[sspec()] + QKV_SPECS + STATE_SPECS * states,
        out_specs=out_specs,
        scratch_shapes=scratch,
        input_output_aliases=alias,
        name=f"attend_{kind}_{int(diag)}{int(forward)}",
        cost_estimate=cost(ATT_FLOPS, 4 << 20, SLAB * NX * HALF),
        compiler_params=pltpu.CompilerParams(dimension_semantics=("arbitrary",)),
    )


def ring(size, step):
    return [(i, (i + step) % size) for i in range(size)]


def body(tokens, wq, wk, wv, wg, fw, fbias, wo):
    z = lax.axis_index("z")
    x = lax.axis_index("x")
    y = lax.axis_index("y")
    c = lax.axis_index("c")
    tp = 2 * y + c

    near = [tokens] + [lax.ppermute(tokens, "y", ring(NY, s)) for s in (1, 2, 3)]
    far = [lax.ppermute(t, "c", ring(NC, 1)) for t in near]
    pos = jnp.stack(
        [2 * ((y + NY - s) % NY) + c for s in range(NY)]
        + [2 * ((y + NY - s) % NY) + 1 - c for s in range(NY)]
    ).astype(jnp.int32)

    mine = lax.dynamic_slice_in_dim(fw, 2 * tp, 2, 1).T
    fwt = jnp.zeros((META, WIDTH), BF).at[:2].set(mine)
    bias = lax.dynamic_slice_in_dim(fbias, 2 * tp, 2, 0)
    bias = jnp.zeros((META, 128), F32).at[:2].set(jnp.broadcast_to(bias[:, None], (2, 128)))

    flops = 2 * BLOCK * WIDTH * COLS
    toks, kx = plain(
        key_kernel, (shape(BLOCK, WIDTH), shape(NX, HALF + META, 128)), 12, "keys", flops, 1
    )(pos, *near, *far, wk, fwt, bias)
    k0 = lax.all_to_all(kx, "x", 0, 0, tiled=True)
    vx = plain(value_kernel, shape(NX, HALF, 128), 2, "values", flops)(toks, wv)
    v0 = lax.all_to_all(vx, "x", 0, 0, tiled=True)
    qx = plain(query_kernel, shape(NX, BLOCK, 128), 2, "queries", flops)(toks, wq)
    q = lax.all_to_all(qx, "x", 0, 0, tiled=True).reshape(SLAB, 128)
    gate = plain(gate_kernel, shape(2, BLOCK, 128, dtype=F32), 2, "gate", flops)(toks, wg)

    fw_ring, bw_ring = ring(NZ, 1), ring(NZ, -1)
    kf, vf, kb, vb = [k0], [v0], [k0], [v0]
    for s in range(1, 5):
        kf.append(lax.ppermute(kf[-1], "z", fw_ring))
        vb.append(lax.ppermute(vb[-1], "z", bw_ring))
        if s < 4:
            vf.append(lax.ppermute(vf[-1], "z", fw_ring))
            kb.append(lax.ppermute(kb[-1], "z", bw_ring))

    half = (x // 2).astype(jnp.int32)

    def flag(valid):
        return jnp.stack([valid.astype(jnp.int32), half])

    front = attention_call("first", diag=True)(flag(z >= 0), q, k0, v0)
    back = None
    for s in range(1, 4):
        front = attention_call("next")(flag(z >= s), q, kf[s], vf[s], *front)
        valid = flag(z + s >= NZ)
        if back is None:
            back = attention_call("first")(valid, q, kb[s], vb[s])
        else:
            back = attention_call("next", forward=False)(valid, q, kb[s], vb[s], *back)
    outs = attention_call("last")(flag(z >= 4), q, kf[4], vb[4], *front, *back)
    parts = lax.all_to_all(outs, "x", 0, 0, tiled=True)
    att = plain(join_kernel, shape(8, PIECE, COLS), 2, "join", 1 << 20)(parts, gate)
    rows = lax.all_to_all(att, ("y", "c"), 0, 0, tiled=True)
    rows = rows.transpose(1, 0, 2).reshape(PIECE, WIDTH)
    return jnp.dot(rows, wo, preferred_element_type=F32).astype(BF)


def solution(mesh):
    axes = ("z", "x", "y", "c")
    grid = Mesh(mesh.devices.reshape(NZ, NX, NY, NC), axes)
    cols = P(None, ("y", "c"))
    return jax.shard_map(
        body,
        mesh=grid,
        in_specs=(P(axes, None), cols, cols, cols, cols, P(), P(), P()),
        out_specs=P(axes, None),
        check_vma=False,
    )
```

```python
import functools

import jax
import jax.numpy as jnp
from jax import lax
from jax.experimental import pallas as pl
from jax.experimental.pallas import tpu as pltpu
from jax.sharding import Mesh
from jax.sharding import PartitionSpec as P

HEAD_DIM = 128
NZ, NX, NY, NC = 8, 4, 4, 2
BLOCK = 512
HALF = 256
SLAB = NX * BLOCK
PIECE = 64
WIDTH = 2048
COLS = 256
META = 16
ROWS = 2 * HALF + META
NEG = -1e30

VMEM = pltpu.VMEM
SMEM = pltpu.SMEM
BF = jnp.bfloat16
F32 = jnp.float32


def vspec():
    return pl.BlockSpec(memory_space=VMEM)


def sspec():
    return pl.BlockSpec(memory_space=SMEM)


def thirds(value):
    high = value.astype(BF).astype(F32)
    rest = value - high
    mid = rest.astype(BF).astype(F32)
    low = (rest - mid).astype(BF).astype(F32)
    return high, mid, low


def kv_kernel(ids_ref, *refs):
    pieces = refs[:8]
    wk_ref, wv_ref, fw_ref, bias_ref, toks_ref, kv_ref, sems, parts_ref = refs[8:]
    y, c = ids_ref[2], ids_ref[3]
    copies = []
    for i in range(8):
        pos = 2 * ((y + NY - i % NY) % NY) + (c if i < NY else 1 - c)
        start = pl.multiple_of(pos * PIECE, PIECE)
        copies.append(
            pltpu.make_async_copy(pieces[i], toks_ref.at[pl.ds(start, PIECE), :], sems.at[i])
        )
    for copy in copies:
        copy.start()
    for copy in copies:
        copy.wait()
    toks = toks_ref[...]
    keys = jnp.dot(toks, wk_ref[...], preferred_element_type=F32).astype(BF)
    values = jnp.dot(toks, wv_ref[...], preferred_element_type=F32).astype(BF)
    logits = lax.dot_general(
        fw_ref[...], toks, (((1,), (1,)), ((), ())), preferred_element_type=F32
    )
    logits = logits + bias_ref[:, :1]
    logs = jnp.minimum(logits, 0.0) - jnp.log1p(jnp.exp(-jnp.abs(logits)))
    row = lax.broadcasted_iota(jnp.int32, (BLOCK, BLOCK), 0)
    col = lax.broadcasted_iota(jnp.int32, (BLOCK, BLOCK), 1)
    upper = (row <= col).astype(BF)
    local = sum(
        jnp.dot(part.astype(BF), upper, preferred_element_type=F32) for part in thirds(logs)
    )
    for i, part in enumerate(thirds(local)):
        parts_ref[i] = part
    for a in range(2):
        head = 2 * (2 * y + c) + a
        mine = [parts_ref[i, pl.ds(head, 1), :] for i in range(3)]
        for b in range(2):
            dest = 2 * b + a
            rows = [
                part[:, b * HALF + i * 128 : b * HALF + (i + 1) * 128]
                for part in mine
                for i in range(2)
            ]
            rows += [jnp.broadcast_to(part[:, BLOCK - 1 :], (1, 128)) for part in mine]
            rows.append(jnp.zeros((META - 9, 128), F32))
            kv_ref[dest, :HALF, :] = keys[b * HALF : (b + 1) * HALF, a * 128 : (a + 1) * 128]
            kv_ref[dest, HALF : 2 * HALF, :] = values[
                b * HALF : (b + 1) * HALF, a * 128 : (a + 1) * 128
            ]
            kv_ref[dest, 2 * HALF :, :] = jnp.concatenate(rows, axis=0).astype(BF)


def query_kernel(toks_ref, wq_ref, wg_ref, qx_ref, gate_ref):
    queries = jnp.dot(toks_ref[...], wq_ref[...], preferred_element_type=F32)
    queries = (queries * HEAD_DIM**-0.5).astype(BF)
    for b in range(2):
        for a in range(2):
            qx_ref[2 * b + a] = queries[:, a * 128 : (a + 1) * 128]
    pre = jnp.dot(toks_ref[...], wg_ref[...], preferred_element_type=F32)
    gate = 1.0 / (1.0 + jnp.exp(-pre))
    for a in range(2):
        gate_ref[a] = gate[:, a * 128 : (a + 1) * 128]


QT = 256
KEYS = NX * HALF
ACC = 144


def fill(blocks, offsets, ka_ref, vt_ref):
    for j, ((ref, index), (rows, before)) in enumerate(zip(blocks, offsets)):
        ka_ref[j * HALF : (j + 1) * HALF, :128] = ref[index, :HALF, :]
        for g in range(2):
            cols = slice(j * HALF + g * 128, j * HALF + (g + 1) * 128)
            parts = thirds(-(rows[g] + before))
            tile = jnp.concatenate([*parts, jnp.zeros((125, 128), F32)], axis=0)
            ka_ref[cols, 128:] = tile.T.astype(BF)
            vals = ref[index, HALF + g * 128 : HALF + (g + 1) * 128, :]
            vt_ref[:128, cols] = vals.astype(F32).T.astype(BF)
    row = lax.broadcasted_iota(jnp.int32, (ACC - 128, KEYS), 0)
    vt_ref[128:, :] = jnp.where(row == 0, 1.0, 0.0).astype(BF)


def slab_offsets(blocks):
    out = []
    before = jnp.zeros((1, 128), F32)
    for ref, index in blocks:
        meta = ref[index, 2 * HALF :, :].astype(F32)
        rows = [meta[i : i + 1] + meta[2 + i : 3 + i] + meta[4 + i : 5 + i] for i in range(2)]
        out.append((rows, before))
        before = before + (meta[6:7] + meta[7:8] + meta[8:9])
    return out, before


def attend(qa_ref, ka_ref, vt_ref, half, old, new):
    m_out, acc_out = new

    def scores(i):
        s = lax.dot_general(
            ka_ref[...],
            qa_ref[i * QT : (i + 1) * QT, :],
            (((1,), (1,)), ((), ())),
            preferred_element_type=F32,
        )
        if half is not None:
            row = lax.broadcasted_iota(jnp.int32, (KEYS, QT), 0)
            col = lax.broadcasted_iota(jnp.int32, (KEYS, QT), 1)
            pos = row + (row // HALF + half) * HALF
            s = jnp.where(pos <= col + i * QT, s, NEG)
        return s

    def finish(i, s):
        cols = slice(i * QT, (i + 1) * QT)
        best = jnp.max(s, axis=0, keepdims=True)
        if old is not None:
            best = jnp.maximum(best, old[0][:1, cols])
        safe = jnp.where(best < -1e29, 0.0, best)
        w = jnp.exp(s - safe).astype(BF)
        acc = jnp.dot(vt_ref[...], w, preferred_element_type=F32)
        if old is not None:
            acc = acc + old[1][:, cols] * jnp.exp(old[0][:1, cols] - safe)
        m_out[:, cols] = jnp.broadcast_to(best, (8, QT))
        acc_out[:, cols] = acc

    s = scores(0)
    for i in range(SLAB // QT):
        following = scores(i + 1) if i + 1 < SLAB // QT else None
        finish(i, s)
        s = following


def whole(ref):
    return [(ref, xs) for xs in range(NX)]


def diag_kernel(ids_ref, q_ref, kv_ref, qa_out, off_out, m_out, acc_out, ka_ref, vt_ref):
    offsets, _ = slab_offsets(whole(kv_ref))
    fill(whole(kv_ref), offsets, ka_ref, vt_ref)
    lane = lax.broadcasted_iota(jnp.int32, (SLAB, 128), 1)
    qa_out[:, :128] = q_ref[...]
    qa_out[:, 128:] = jnp.where(lane < 3, 1.0, 0.0).astype(BF)
    attend(qa_out, ka_ref, vt_ref, ids_ref[1] // 2, None, (m_out, acc_out))
    off_out[...] = jnp.zeros((8, 128), F32)


def shifted(offsets, base):
    return [(rows, before + base) for rows, before in offsets]


def front_kernel(
    step, ids_ref, qa_ref, kv_ref, off_in, m_in, acc_in, off_out, m_out, acc_out, ka_ref, vt_ref
):
    valid = ids_ref[0] >= step

    @pl.when(valid)
    def _():
        offsets, total = slab_offsets(whole(kv_ref))
        base = off_in[:1, :] - total
        fill(whole(kv_ref), shifted(offsets, base), ka_ref, vt_ref)
        attend(qa_ref, ka_ref, vt_ref, None, (m_in, acc_in), (m_out, acc_out))
        off_out[...] = jnp.broadcast_to(base, (8, 128))

    @pl.when(jnp.logical_not(valid))
    def _():
        off_out[...] = off_in[...]
        m_out[...] = m_in[...]
        acc_out[...] = acc_in[...]


def back_kernel(step, ids_ref, qa_ref, kv_ref, *refs):
    ins, (off_out, m_out, acc_out, ka_ref, vt_ref) = refs[:-5], refs[-5:]
    valid = ids_ref[0] + step >= NZ

    @pl.when(valid)
    def _():
        offsets, total = slab_offsets(whole(kv_ref))
        base = ins[0][:1, :] if ins else jnp.zeros((1, 128), F32)
        fill(whole(kv_ref), shifted(offsets, base), ka_ref, vt_ref)
        old = (ins[1], ins[2]) if ins else None
        attend(qa_ref, ka_ref, vt_ref, None, old, (m_out, acc_out))
        off_out[...] = jnp.broadcast_to(base + total, (8, 128))

    @pl.when(jnp.logical_not(valid))
    def _():
        if ins:
            off_out[...] = ins[0][...]
            m_out[...] = ins[1][...]
            acc_out[...] = ins[2][...]
        else:
            off_out[...] = jnp.zeros((8, 128), F32)
            m_out[...] = jnp.full((8, SLAB), NEG, F32)
            acc_out[...] = jnp.zeros((ACC, SLAB), F32)


def last_kernel(
    ids_ref, qa_ref, kv0_ref, kv1_ref, foff, fm, facc, boff, bm, bacc, out_ref,
    off_s, m_s, acc_s, ka_ref, vt_ref,
):
    valid = ids_ref[0] >= 4
    blocks = [(kv0_ref, 0), (kv0_ref, 1), (kv1_ref, 0), (kv1_ref, 1)]

    @pl.when(valid)
    def _():
        offsets, total = slab_offsets(blocks)
        base = foff[:1, :] - total
        fill(blocks, shifted(offsets, base), ka_ref, vt_ref)
        attend(qa_ref, ka_ref, vt_ref, None, (fm, facc), (m_s, acc_s))
        off_s[...] = jnp.broadcast_to(base, (8, 128))

    @pl.when(jnp.logical_not(valid))
    def _():
        off_s[...] = foff[...]
        m_s[...] = fm[...]
        acc_s[...] = facc[...]

    shift = (boff[:1, :] - off_s[:1, :])[:, :1]
    for i in range(NX):
        cols = slice(i * BLOCK, (i + 1) * BLOCK)
        best_f = m_s[:1, cols]
        best_b = jnp.where(bacc[128:129, cols] > 0.0, bm[:1, cols] + shift, NEG)
        best = jnp.maximum(best_f, best_b)
        safe = jnp.where(best < -1e29, 0.0, best)
        wf = jnp.exp(best_f - safe)
        wb = jnp.exp(best_b - safe)
        total = wf * acc_s[128:129, cols] + wb * bacc[128:129, cols]
        some = total > 0.0
        inverse = 1.0 / jnp.where(some, total, 1.0)
        wf = wf * inverse
        wb = wb * inverse
        mix = wf * acc_s[:128, cols] + wb * bacc[:128, cols]
        for g in range(BLOCK // 128):
            out_ref[i, g * 128 : (g + 1) * 128, :] = mix[:, g * 128 : (g + 1) * 128].T.astype(BF)
        lse = jnp.where(some, best + jnp.log(jnp.where(some, total, 1.0)), NEG)
        stats = jnp.concatenate([lse[:, g * 128 : (g + 1) * 128] for g in range(4)], axis=0)
        rows = jnp.concatenate([*thirds(stats), jnp.zeros((META - 12, 128), F32)], axis=0)
        out_ref[i, BLOCK:, :] = rows.astype(BF)

def join_kernel(part_ref, gate_ref, out_ref):
    for a in range(2):
        lses = []
        for b in range(2):
            meta = part_ref[2 * b + a, BLOCK:, :].astype(F32)
            lses.append(meta[0:4] + meta[4:8] + meta[8:12])
        for g in range(4):
            rows = slice(g * 128, (g + 1) * 128)
            l0, l1 = [jnp.broadcast_to(lse[g : g + 1], (128, 128)).T for lse in lses]
            best = jnp.maximum(l0, l1)
            w0 = jnp.exp(l0 - best)
            w1 = jnp.exp(l1 - best)
            mix = w0 * part_ref[a, rows, :].astype(F32) + w1 * part_ref[2 + a, rows, :].astype(F32)
            att = (mix / (w0 + w1) * gate_ref[a, rows, :]).astype(BF)
            for h in range(2):
                out_ref[2 * g + h, :, a * 128 : (a + 1) * 128] = att[h * PIECE : (h + 1) * PIECE]


def out_kernel(rows_ref, wo_ref, out_ref, lhs_ref):
    for j in range(NY * NC):
        lhs_ref[:, j * COLS : (j + 1) * COLS] = rows_ref[j]
    out_ref[...] = jnp.dot(lhs_ref[...], wo_ref[...], preferred_element_type=F32).astype(BF)


def shape(*dims, dtype=BF):
    return jax.ShapeDtypeStruct(dims, dtype)


def call(kernel, outs, specs, name, flops, scratch=(), alias=None, mib=16, exps=0):
    return pl.pallas_call(
        kernel,
        out_shape=outs,
        in_specs=specs,
        out_specs=jax.tree.map(lambda _: vspec(), outs),
        scratch_shapes=scratch,
        input_output_aliases=alias or {},
        name=name,
        cost_estimate=pl.CostEstimate(
            flops=flops, bytes_accessed=2 << 20, transcendentals=exps
        ),
        compiler_params=pltpu.CompilerParams(vmem_limit_bytes=mib << 20),
    )


STATE = (shape(8, 128, dtype=F32), shape(8, SLAB, dtype=F32), shape(ACC, SLAB, dtype=F32))
LOADED = [VMEM((KEYS, 256), BF), VMEM((ACC, KEYS), BF)]


def attention(kernel, outs, n_in, name, alias=None, scratch=()):
    specs = [sspec()] + [vspec()] * (n_in - 1)
    flops = 4 * SLAB * KEYS * 128
    return call(
        kernel, outs, specs, name, flops, [*scratch, *LOADED], alias, 28, SLAB * KEYS
    )


def ring(size, step):
    return [(i, (i + step) % size) for i in range(size)]


def body(tokens, wq, wk, wv, wg, fw, fbias, wo):
    ids = jnp.stack([lax.axis_index(a) for a in AXES]).astype(jnp.int32)
    fwt = fw.T
    bias = jnp.broadcast_to(fbias[:, None], (16, 128))

    near = [tokens] + [lax.ppermute(tokens, "y", ring(NY, s)) for s in (1, 2, 3)]
    far = [lax.ppermute(t, "c", ring(NC, 1)) for t in near]
    flops = 2 * BLOCK * WIDTH * COLS
    toks, kvx = call(
        kv_kernel,
        (shape(BLOCK, WIDTH), shape(NX, ROWS, 128)),
        [sspec()] + [pl.BlockSpec(memory_space=pltpu.HBM)] * 8 + [vspec()] * 4,
        "keys_values",
        2 * flops,
        [pltpu.SemaphoreType.DMA((8,)), VMEM((3, 16, BLOCK), F32)],
    )(ids, *near, *far, wk, wv, fwt, bias)
    kv = lax.all_to_all(kvx, "x", 0, 0, tiled=True)
    qx, gate = call(
        query_kernel,
        (shape(NX, BLOCK, 128), shape(2, BLOCK, 128, dtype=F32)),
        [vspec()] * 3,
        "queries_gate",
        2 * flops,
    )(toks, wq, wg)
    q = lax.all_to_all(qx, "x", 0, 0, tiled=True).reshape(SLAB, 128)

    kf, kb = [kv], [kv]
    for s in range(1, 4):
        kf.append(lax.ppermute(kf[-1], "z", ring(NZ, 1)))
        kb.append(lax.ppermute(kb[-1], "z", ring(NZ, -1)))
    far0 = lax.ppermute(kf[3][:2], "z", ring(NZ, 1))
    far1 = lax.ppermute(kb[3][2:], "z", ring(NZ, -1))

    qa, *front = attention(diag_kernel, (shape(SLAB, 256), *STATE), 3, "attend_own")(ids, q, kv)
    back = []
    for s in range(1, 4):
        front = attention(
            functools.partial(front_kernel, s), STATE, 6, f"attend_front_{s}", {3: 0, 4: 1, 5: 2}
        )(ids, qa, kf[s], *front)
        back = attention(
            functools.partial(back_kernel, s), STATE, 3 + len(back), f"attend_back_{s}",
            {3: 0, 4: 1, 5: 2} if back else None,
        )(ids, qa, kb[s], *back)
    outs = attention(
        last_kernel, shape(NX, BLOCK + META, 128), 10, "attend_last", None,
        [VMEM(s.shape, F32) for s in STATE],
    )(ids, qa, far0, far1, *front, *back)
    parts = lax.all_to_all(outs, "x", 0, 0, tiled=True)
    att = call(join_kernel, shape(NY * NC, PIECE, COLS), [vspec()] * 2, "join", 1 << 20)(
        parts, gate
    )
    rows = lax.all_to_all(att, ("y", "c"), 0, 0, tiled=True)
    return call(
        out_kernel, shape(PIECE, WIDTH), [vspec()] * 2, "project", 2 * PIECE * WIDTH * WIDTH,
        [VMEM((PIECE, WIDTH), BF)],
    )(rows, wo)


AXES = ("z", "x", "y", "c")


def solution(mesh):
    grid = Mesh(mesh.devices.reshape(NZ, NX, NY, NC), AXES)
    cols = P(None, ("y", "c"))
    return jax.shard_map(
        body,
        mesh=grid,
        in_specs=(P(AXES, None), cols, cols, cols, cols, P(), P(), P()),
        out_specs=P(AXES, None),
        check_vma=False,
    )
```

```python
import functools

import jax
import jax.numpy as jnp
from jax import lax
from jax.experimental import pallas as pl
from jax.experimental.pallas import tpu as pltpu
from jax.sharding import Mesh
from jax.sharding import PartitionSpec as P


HEAD_DIM = 128
NZ, NX, NY, NC = 8, 4, 4, 2
BLOCK = 512
HALF = 256
SLAB = NX * BLOCK
PIECE = 64
WIDTH = 2048
COLS = 256
META = 16
ROWS = 2 * HALF + META
NEG = -1e30

VMEM = pltpu.VMEM
SMEM = pltpu.SMEM
BF = jnp.bfloat16
F32 = jnp.float32


def vspec():
    return pl.BlockSpec(memory_space=VMEM)


def sspec():
    return pl.BlockSpec(memory_space=SMEM)


def thirds(value):
    high = value.astype(BF).astype(F32)
    rest = value - high
    mid = rest.astype(BF).astype(F32)
    low = (rest - mid).astype(BF).astype(F32)
    return high, mid, low


def gather(ids_ref, pieces, toks_ref, weights, sems):
    y, c = ids_ref[2], ids_ref[3]
    parts = 4
    pairs = []
    for source, target in weights:
        for i in range(parts):
            rows = pl.ds(i * WIDTH // parts, WIDTH // parts)
            pairs.append((source.at[rows, :], target.at[rows, :]))
    for i in range(8):
        pos = 2 * ((y + NY - i % NY) % NY) + (c if i < NY else 1 - c)
        start = pl.multiple_of(pos * PIECE, PIECE)
        pairs.append((pieces[i], toks_ref.at[pl.ds(start, PIECE), :]))
    copies = [
        pltpu.make_async_copy(source, target, sems.at[i])
        for i, (source, target) in enumerate(pairs)
    ]
    for copy in copies:
        copy.start()
    for copy in copies:
        copy.wait()
    return toks_ref[...]


def kv_kernel(ids_ref, *refs):
    wk_hbm, wv_hbm, fw_ref, bias_ref, kv_ref, toks_ref, wk_ref, wv_ref, sems, parts_ref = refs[8:]
    y, c = ids_ref[2], ids_ref[3]
    weights = [(wk_hbm, wk_ref), (wv_hbm, wv_ref)]
    toks = gather(ids_ref, refs[:8], toks_ref, weights, sems)
    keys = jnp.dot(toks, wk_ref[...], preferred_element_type=F32).astype(BF)
    values = jnp.dot(toks, wv_ref[...], preferred_element_type=F32).astype(BF)
    logits = lax.dot_general(
        fw_ref[...], toks, (((1,), (1,)), ((), ())), preferred_element_type=F32
    )
    row = lax.broadcasted_iota(jnp.int32, (16, BLOCK), 0)
    for head in range(16):
        logits = logits + jnp.where(row == head, bias_ref[head], 0.0)
    logs = jnp.minimum(logits, 0.0) - jnp.log1p(jnp.exp(-jnp.abs(logits)))
    row = lax.broadcasted_iota(jnp.int32, (BLOCK, BLOCK), 0)
    col = lax.broadcasted_iota(jnp.int32, (BLOCK, BLOCK), 1)
    upper = (row <= col).astype(BF)
    local = sum(
        jnp.dot(part.astype(BF), upper, preferred_element_type=F32) for part in thirds(logs)
    )
    for i, part in enumerate(thirds(local)):
        parts_ref[i] = part
    for a in range(2):
        head = 2 * (2 * y + c) + a
        mine = [parts_ref[i, pl.ds(head, 1), :] for i in range(3)]
        for b in range(2):
            dest = 2 * b + a
            rows = [
                part[:, b * HALF + i * 128 : b * HALF + (i + 1) * 128]
                for part in mine
                for i in range(2)
            ]
            rows += [jnp.broadcast_to(part[:, BLOCK - 1 :], (1, 128)) for part in mine]
            rows.append(jnp.zeros((META - 9, 128), F32))
            kv_ref[dest, :HALF, :] = keys[b * HALF : (b + 1) * HALF, a * 128 : (a + 1) * 128]
            kv_ref[dest, HALF : 2 * HALF, :] = values[
                b * HALF : (b + 1) * HALF, a * 128 : (a + 1) * 128
            ]
            kv_ref[dest, 2 * HALF :, :] = jnp.concatenate(rows, axis=0).astype(BF)


def query_kernel(ids_ref, *refs):
    wq_hbm, wg_hbm, qx_ref, gate_ref, toks_ref, wq_ref, wg_ref, sems = refs[8:]
    weights = [(wq_hbm, wq_ref), (wg_hbm, wg_ref)]
    toks = gather(ids_ref, refs[:8], toks_ref, weights, sems)
    queries = jnp.dot(toks, wq_ref[...], preferred_element_type=F32)
    queries = (queries * HEAD_DIM**-0.5).astype(BF)
    for b in range(2):
        for a in range(2):
            qx_ref[2 * b + a] = queries[:, a * 128 : (a + 1) * 128]
    pre = jnp.dot(toks, wg_ref[...], preferred_element_type=F32)
    gate = 1.0 / (1.0 + jnp.exp(-pre))
    for a in range(2):
        gate_ref[a] = gate[:, a * 128 : (a + 1) * 128]


def arrived_kernel(ids_ref, front_ref, back_ref, out_ref):
    for i in range(4):
        out_ref[i] = ids_ref[i]


QT = 256
KEYS = NX * HALF
TILES = SLAB // QT
ACC = 144


def fill(blocks, offsets, ka_ref, vt_ref):
    for j, ((ref, index), (rows, before)) in enumerate(zip(blocks, offsets)):
        ka_ref[j * HALF : (j + 1) * HALF, :128] = ref[index, :HALF, :]
        for g in range(2):
            cols = slice(j * HALF + g * 128, j * HALF + (g + 1) * 128)
            parts = thirds(-(rows[g] + before))
            tile = jnp.concatenate([*parts, jnp.zeros((125, 128), F32)], axis=0)
            ka_ref[cols, 128:] = tile.T.astype(BF)
            vals = ref[index, HALF + g * 128 : HALF + (g + 1) * 128, :]
            vt_ref[:128, cols] = vals.astype(F32).T.astype(BF)
    row = lax.broadcasted_iota(jnp.int32, (ACC - 128, KEYS), 0)
    vt_ref[128:, :] = jnp.where(row == 0, 1.0, 0.0).astype(BF)


def slab_offsets(blocks):
    out = []
    before = jnp.zeros((1, 128), F32)
    for ref, index in blocks:
        meta = ref[index, 2 * HALF :, :].astype(F32)
        rows = [meta[i : i + 1] + meta[2 + i : 3 + i] + meta[4 + i : 5 + i] for i in range(2)]
        out.append((rows, before))
        before = before + (meta[6:7] + meta[7:8] + meta[8:9])
    return out, before


def attend(qa_ref, ka_ref, vt_ref, half, old, new):
    m_out, acc_out = new

    def scores(i, keys):
        start = i * QT if half is not None else pl.multiple_of(i * QT, QT)
        s = lax.dot_general(
            ka_ref[:keys, :],
            qa_ref[pl.ds(start, QT), :],
            (((1,), (1,)), ((), ())),
            preferred_element_type=F32,
        )
        if half is not None:
            row = lax.broadcasted_iota(jnp.int32, (keys, QT), 0)
            col = lax.broadcasted_iota(jnp.int32, (keys, QT), 1)
            pos = row + (row // HALF + half) * HALF
            s = jnp.where(pos <= col + start, s, NEG)
        return s

    def finish(i, keys, s):
        best = jnp.max(s, axis=0, keepdims=True)
        if old is not None:
            before = old[0][i][:1]
            best = jnp.maximum(best, before)
        safe = jnp.where(best < -1e29, 0.0, best)
        w = jnp.exp(s - safe).astype(BF)
        acc = jnp.dot(vt_ref[:, :keys], w, preferred_element_type=F32)
        if old is not None:
            acc = acc + old[1][i] * jnp.exp(before - safe)
        m_out[i] = jnp.broadcast_to(best, (8, QT))
        acc_out[i] = acc

    def run(tiles):
        s = scores(*tiles[0])
        for tile, after in zip(tiles, [*tiles[1:], None]):
            following = scores(*after) if after else None
            finish(*tile, s)
            s = following

    if half is not None:
        run([(i, HALF * (i * QT // BLOCK + 1)) for i in range(TILES)])
    else:
        part = TILES // 2

        def some(j, carry):
            run([(j * part + i, KEYS) for i in range(part)])
            return carry

        lax.fori_loop(0, 2, some, 0)


def whole(ref):
    return [(ref, xs) for xs in range(NX)]


def diag_kernel(ids_ref, q_ref, kv_ref, qa_out, off_out, m_out, acc_out, ka_ref, vt_ref):
    offsets, _ = slab_offsets(whole(kv_ref))
    fill(whole(kv_ref), offsets, ka_ref, vt_ref)
    lane = lax.broadcasted_iota(jnp.int32, (SLAB, 128), 1)
    qa_out[:, :128] = q_ref[...]
    qa_out[:, 128:] = jnp.where(lane < 3, 1.0, 0.0).astype(BF)
    attend(qa_out, ka_ref, vt_ref, ids_ref[1] // 2, None, (m_out, acc_out))
    off_out[...] = jnp.zeros((8, 128), F32)


def shifted(offsets, base):
    return [(rows, before + base) for rows, before in offsets]


def front_kernel(
    step, ids_ref, qa_ref, kv_ref, off_in, m_in, acc_in, off_out, m_out, acc_out, ka_ref, vt_ref
):
    valid = ids_ref[0] >= step

    @pl.when(valid)
    def _():
        offsets, total = slab_offsets(whole(kv_ref))
        base = off_in[:1, :] - total
        fill(whole(kv_ref), shifted(offsets, base), ka_ref, vt_ref)
        attend(qa_ref, ka_ref, vt_ref, None, (m_in, acc_in), (m_out, acc_out))
        off_out[...] = jnp.broadcast_to(base, (8, 128))

    @pl.when(jnp.logical_not(valid))
    def _():
        off_out[...] = off_in[...]
        m_out[...] = m_in[...]
        acc_out[...] = acc_in[...]


def back_kernel(step, ids_ref, qa_ref, kv_ref, *refs):
    ins, (off_out, m_out, acc_out, ka_ref, vt_ref) = refs[:-5], refs[-5:]
    valid = ids_ref[0] + step >= NZ

    @pl.when(valid)
    def _():
        offsets, total = slab_offsets(whole(kv_ref))
        base = ins[0][:1, :] if ins else jnp.zeros((1, 128), F32)
        fill(whole(kv_ref), shifted(offsets, base), ka_ref, vt_ref)
        old = (ins[1], ins[2]) if ins else None
        attend(qa_ref, ka_ref, vt_ref, None, old, (m_out, acc_out))
        off_out[...] = jnp.broadcast_to(base + total, (8, 128))

    @pl.when(jnp.logical_not(valid))
    def _():
        if ins:
            off_out[...] = ins[0][...]
            m_out[...] = ins[1][...]
            acc_out[...] = ins[2][...]
        else:
            off_out[...] = jnp.zeros((8, 128), F32)
            m_out[...] = jnp.full(m_out.shape, NEG, F32)
            acc_out[...] = jnp.zeros(acc_out.shape, F32)


def last_kernel(
    ids_ref, qa_ref, kv0_ref, kv1_ref, foff, fm, facc, boff, bm, bacc, out_ref,
    off_s, m_s, acc_s, ka_ref, vt_ref,
):
    valid = ids_ref[0] >= 4
    blocks = [(kv0_ref, 0), (kv0_ref, 1), (kv1_ref, 0), (kv1_ref, 1)]

    @pl.when(valid)
    def _():
        offsets, total = slab_offsets(blocks)
        base = foff[:1, :] - total
        fill(blocks, shifted(offsets, base), ka_ref, vt_ref)
        attend(qa_ref, ka_ref, vt_ref, None, (fm, facc), (m_s, acc_s))
        off_s[...] = jnp.broadcast_to(base, (8, 128))

    @pl.when(jnp.logical_not(valid))
    def _():
        off_s[...] = foff[...]
        m_s[...] = fm[...]
        acc_s[...] = facc[...]

    shift = (boff[:1, :] - off_s[:1, :])[:, :1]
    stats = []
    for i in range(TILES):
        best_f = m_s[i, :1, :]
        best_b = jnp.where(bacc[i, 128:129, :] > 0.0, bm[i, :1, :] + shift, NEG)
        best = jnp.maximum(best_f, best_b)
        safe = jnp.where(best < -1e29, 0.0, best)
        wf = jnp.exp(best_f - safe)
        wb = jnp.exp(best_b - safe)
        total = wf * acc_s[i, 128:129, :] + wb * bacc[i, 128:129, :]
        some = total > 0.0
        total = jnp.where(some, total, 1.0)
        wf = wf / total
        wb = wb / total
        mix = wf * acc_s[i, :128, :] + wb * bacc[i, :128, :]
        lse = jnp.where(some, best + jnp.log(total), NEG)
        for g in range(QT // 128):
            row = i * QT % BLOCK + g * 128
            tile = mix[:, g * 128 : (g + 1) * 128].T
            out_ref[i * QT // BLOCK, row : row + 128, :] = tile.astype(BF)
            stats.append(lse[:, g * 128 : (g + 1) * 128])
    for i in range(NX):
        part = jnp.concatenate(stats[4 * i : 4 * i + 4], axis=0)
        rows = jnp.concatenate([*thirds(part), jnp.zeros((META - 12, 128), F32)], axis=0)
        out_ref[i, BLOCK:, :] = rows.astype(BF)


def join_kernel(part_ref, gate_ref, out_ref):
    for a in range(2):
        lses = []
        for b in range(2):
            meta = part_ref[2 * b + a, BLOCK:, :].astype(F32)
            lses.append(meta[0:4] + meta[4:8] + meta[8:12])
        share = 1.0 / (1.0 + jnp.exp(lses[1] - lses[0]))
        for g in range(4):
            rows = slice(g * 128, (g + 1) * 128)
            w0 = jnp.broadcast_to(share[g : g + 1], (128, 128)).T
            p0 = part_ref[a, rows, :].astype(F32)
            p1 = part_ref[2 + a, rows, :].astype(F32)
            att = ((w0 * p0 + (1.0 - w0) * p1) * gate_ref[a, rows, :]).astype(BF)
            for h in range(2):
                out_ref[2 * g + h, :, a * 128 : (a + 1) * 128] = att[h * PIECE : (h + 1) * PIECE]


def out_kernel(rows_ref, wo_ref, out_ref, lhs_ref):
    for j in range(NY * NC):
        lhs_ref[:, j * COLS : (j + 1) * COLS] = rows_ref[j]
    out_ref[...] = jnp.dot(lhs_ref[...], wo_ref[...], preferred_element_type=F32).astype(BF)


def shape(*dims, dtype=BF):
    return jax.ShapeDtypeStruct(dims, dtype)


def call(kernel, outs, specs, flops, scratch=(), alias=None, mib=16, exps=0):
    return pl.pallas_call(
        kernel,
        out_shape=outs,
        in_specs=specs,
        out_specs=jax.tree.map(lambda _: vspec(), outs),
        scratch_shapes=scratch,
        input_output_aliases=alias or {},
        cost_estimate=pl.CostEstimate(
            flops=flops, bytes_accessed=2 << 20, transcendentals=exps
        ),
        compiler_params=pltpu.CompilerParams(vmem_limit_bytes=mib << 20),
    )


STATE = (
    shape(8, 128, dtype=F32),
    shape(TILES, 8, QT, dtype=F32),
    shape(TILES, ACC, QT, dtype=F32),
)
LOADED = [VMEM((KEYS, 256), BF), VMEM((ACC, KEYS), BF)]


def attention(kernel, outs, n_in, alias=None, scratch=()):
    specs = [sspec()] + [vspec()] * (n_in - 1)
    flops = 4 * SLAB * KEYS * 128
    return call(kernel, outs, specs, flops, [*scratch, *LOADED], alias, 28, SLAB * KEYS)


def ring(size, step):
    return [(i, (i + step) % size) for i in range(size)]


def body(tokens, wq, wk, wv, wg, fw, fbias, wo):
    ids = jnp.stack([lax.axis_index(a) for a in AXES]).astype(jnp.int32)

    near = [tokens] + [lax.ppermute(tokens, "y", ring(NY, s)) for s in (1, 2, 3)]
    far = [lax.ppermute(t, "c", ring(NC, 1)) for t in near]
    flops = 2 * BLOCK * WIDTH * COLS
    hbm = pl.BlockSpec(memory_space=pltpu.HBM)
    room = [
        VMEM((BLOCK, WIDTH), BF),
        VMEM((WIDTH, COLS), BF),
        VMEM((WIDTH, COLS), BF),
        pltpu.SemaphoreType.DMA((16,)),
    ]
    kvx = call(
        kv_kernel,
        shape(NX, ROWS, 128),
        [sspec()] + [hbm] * 10 + [vspec(), sspec()],
        2 * flops,
        [*room, VMEM((3, 16, BLOCK), F32)],
        mib=60,
    )(ids, *near, *far, wk, wv, fw.T, fbias)
    kv = lax.all_to_all(kvx, "x", 0, 0, tiled=True)
    qx, gate = call(
        query_kernel,
        (shape(NX, BLOCK, 128), shape(2, BLOCK, 128, dtype=F32)),
        [sspec()] + [hbm] * 10,
        2 * flops,
        room,
        mib=60,
    )(ids, *near, *far, wq, wg)
    q = lax.all_to_all(qx, "x", 0, 0, tiled=True).reshape(SLAB, 128)

    def hop(value, direction):
        return lax.ppermute(value, "z", ring(NZ, direction))

    kf, kb = [kv], [kv]
    for _ in range(1, 4):
        kf.append(hop(kf[-1], 1))
        kb.append(hop(kb[-1], -1))
    far0 = hop(kf[3][:2], 1)
    far1 = hop(kb[3][2:], -1)

    ids = pl.pallas_call(
        arrived_kernel,
        out_shape=shape(4, dtype=jnp.int32),
        in_specs=[sspec(), hbm, hbm],
        out_specs=sspec(),
        name="arrived",
    )(ids, kf[1], kb[1])
    qa, *front = attention(diag_kernel, (shape(SLAB, 256), *STATE), 3)(ids, q, kv)
    back = []
    for s in range(1, 4):
        back = attention(
            functools.partial(back_kernel, s), STATE, 3 + len(back),
            {3: 0, 4: 1, 5: 2} if back else None,
        )(ids, qa, kb[s], *back)
        front = attention(
            functools.partial(front_kernel, s), STATE, 6, {3: 0, 4: 1, 5: 2}
        )(ids, qa, kf[s], *front)
    outs = attention(
        last_kernel, shape(NX, BLOCK + META, 128), 10, None, [VMEM(s.shape, F32) for s in STATE]
    )(ids, qa, far0, far1, *front, *back)
    parts = lax.all_to_all(outs, "x", 0, 0, tiled=True)
    att = call(join_kernel, shape(NY * NC, PIECE, COLS), [vspec()] * 2, 1 << 20)(parts, gate)
    rows = lax.all_to_all(att, ("y", "c"), 0, 0, tiled=True)
    return call(
        out_kernel, shape(PIECE, WIDTH), [vspec()] * 2, 2 * PIECE * WIDTH * WIDTH,
        [VMEM((PIECE, WIDTH), BF)],
    )(rows, wo)


AXES = ("z", "x", "y", "c")


def solution(mesh):
    grid = Mesh(mesh.devices.reshape(NZ, NX, NY, NC), AXES)
    cols = P(None, ("y", "c"))

    return jax.shard_map(
        body,
        mesh=grid,
        in_specs=(P(AXES, None), cols, cols, cols, cols, P(), P(), P()),
        out_specs=P(AXES, None),
        check_vma=False,
    )
```

```python
import functools

import jax
import jax.numpy as jnp
from jax import lax
from jax.experimental import pallas as pl
from jax.experimental.pallas import tpu as pltpu
from jax.sharding import Mesh
from jax.sharding import PartitionSpec as P


HEAD_DIM = 128
NZ, NX, NY, NC = 8, 4, 4, 2
BLOCK = 512
HALF = 256
SLAB = NX * BLOCK
PIECE = 64
WIDTH = 2048
COLS = 256
META = 16
ROWS = 2 * HALF + META
NEG = -1e30

VMEM = pltpu.VMEM
SMEM = pltpu.SMEM
BF = jnp.bfloat16
F32 = jnp.float32


def vspec():
    return pl.BlockSpec(memory_space=VMEM)


def sspec():
    return pl.BlockSpec(memory_space=SMEM)


def thirds(value):
    high = value.astype(BF).astype(F32)
    rest = value - high
    mid = rest.astype(BF).astype(F32)
    low = (rest - mid).astype(BF).astype(F32)
    return high, mid, low


def fetch(ids_ref, pieces, toks_ref, weights, sems):
    y, c = ids_ref[2], ids_ref[3]
    pairs = []
    for i in range(8):
        pos = 2 * ((y + NY - i % NY) % NY) + (c if i < NY else 1 - c)
        start = pl.multiple_of(pos * PIECE, PIECE)
        pairs.append((pieces[i], toks_ref.at[pl.ds(start, PIECE), :]))
    parts = 4
    for source, target in weights:
        for i in range(parts):
            rows = pl.ds(i * WIDTH // parts, WIDTH // parts)
            pairs.append((source.at[rows, :], target.at[rows, :]))
    copies = [
        pltpu.make_async_copy(source, target, sems.at[i])
        for i, (source, target) in enumerate(pairs)
    ]
    for copy in copies:
        copy.start()
    return copies[:8], copies[8:]


def wait_all(copies):
    for copy in copies:
        copy.wait()


def kv_kernel(ids_ref, *refs):
    wk_hbm, wv_hbm, fw_ref, bias_ref, kv_ref, toks_ref, wk_ref, wv_ref, sems, parts_ref = refs[8:]
    y, c = ids_ref[2], ids_ref[3]
    weights = [(wk_hbm, wk_ref), (wv_hbm, wv_ref)]
    toks_copies, weight_copies = fetch(ids_ref, refs[:8], toks_ref, weights, sems)
    wait_all(toks_copies)
    toks = toks_ref[...]
    logits = lax.dot_general(
        fw_ref[...], toks, (((1,), (1,)), ((), ())), preferred_element_type=F32
    )
    row = lax.broadcasted_iota(jnp.int32, (16, BLOCK), 0)
    for head in range(16):
        logits = logits + jnp.where(row == head, bias_ref[head], 0.0)
    logs = jnp.minimum(logits, 0.0) - jnp.log1p(jnp.exp(-jnp.abs(logits)))
    row = lax.broadcasted_iota(jnp.int32, (BLOCK, BLOCK), 0)
    col = lax.broadcasted_iota(jnp.int32, (BLOCK, BLOCK), 1)
    upper = (row <= col).astype(BF)
    local = sum(
        jnp.dot(part.astype(BF), upper, preferred_element_type=F32) for part in thirds(logs)
    )
    for i, part in enumerate(thirds(local)):
        parts_ref[i] = part
    wait_all(weight_copies)
    keys = jnp.dot(toks, wk_ref[...], preferred_element_type=F32).astype(BF)
    values = jnp.dot(toks, wv_ref[...], preferred_element_type=F32)
    for a in range(2):
        head = 2 * (2 * y + c) + a
        mine = [parts_ref[i, pl.ds(head, 1), :] for i in range(3)]
        for b in range(2):
            dest = 2 * b + a
            rows = [
                part[:, b * HALF + i * 128 : b * HALF + (i + 1) * 128]
                for part in mine
                for i in range(2)
            ]
            rows += [jnp.broadcast_to(part[:, BLOCK - 1 :], (1, 128)) for part in mine]
            rows.append(jnp.zeros((META - 9, 128), F32))
            kv_ref[dest, :HALF, :] = keys[b * HALF : (b + 1) * HALF, a * 128 : (a + 1) * 128]
            for g in range(2):
                tile = values[b * HALF + g * 128 : b * HALF + (g + 1) * 128, a * 128 : (a + 1) * 128]
                kv_ref[dest, HALF + g * 128 : HALF + (g + 1) * 128, :] = tile.T.astype(BF)
            kv_ref[dest, 2 * HALF :, :] = jnp.concatenate(rows, axis=0).astype(BF)


def by_parity(ids_ref, both):
    even = ids_ref[1] % 2 == 0
    low, high = both[:, :128], both[:, 128:]
    return jnp.where(even, low, high), jnp.where(even, high, low)


def query_kernel(ids_ref, *refs):
    wq_hbm, same_ref, other_ref, toks_ref, wq_ref, sems = refs[8:]
    toks_copies, weight_copies = fetch(ids_ref, refs[:8], toks_ref, [(wq_hbm, wq_ref)], sems)
    wait_all(toks_copies + weight_copies)
    queries = jnp.dot(toks_ref[...], wq_ref[...], preferred_element_type=F32)
    same, other = by_parity(ids_ref, queries * HEAD_DIM**-0.5)
    same_ref[...] = same.astype(BF)
    other_ref[...] = other.astype(BF)


def gate_kernel(ids_ref, *refs):
    wg_hbm, gate_ref, toks_ref, wg_ref, sems = refs[8:]
    toks_copies, weight_copies = fetch(ids_ref, refs[:8], toks_ref, [(wg_hbm, wg_ref)], sems)
    wait_all(toks_copies + weight_copies)
    pre = jnp.dot(toks_ref[...], wg_ref[...], preferred_element_type=F32)
    gate_ref[0], gate_ref[1] = by_parity(ids_ref, 1.0 / (1.0 + jnp.exp(-pre)))


QT = 256
KEYS = NX * HALF
TILES = SLAB // QT
ACC = 144


def fill(blocks, offsets, ka_ref, vt_ref):
    biases = [rows[g] + before for rows, before in offsets for g in range(2)]
    parts = thirds(-jnp.concatenate(biases, axis=0))
    turned = jnp.concatenate([*parts, jnp.zeros((104, 128), F32)], axis=0).T
    lane = lax.broadcasted_iota(jnp.int32, (128, 128), 1)
    for j, (ref, index) in enumerate(blocks):
        ka_ref[j * HALF : (j + 1) * HALF, :128] = ref[index, :HALF, :]
        for g in range(2):
            cols = slice(j * HALF + g * 128, j * HALF + (g + 1) * 128)
            ka_ref[cols, 128:] = jnp.where(lane % 8 == 2 * j + g, turned, 0.0).astype(BF)
            vt_ref[:128, cols] = ref[index, HALF + g * 128 : HALF + (g + 1) * 128, :]
    row = lax.broadcasted_iota(jnp.int32, (ACC - 128, KEYS), 0)
    vt_ref[128:, :] = jnp.where(row == 0, 1.0, 0.0).astype(BF)


def slab_offsets(blocks):
    out = []
    before = jnp.zeros((1, 128), F32)
    for ref, index in blocks:
        meta = ref[index, 2 * HALF :, :].astype(F32)
        rows = [meta[i : i + 1] + meta[2 + i : 3 + i] + meta[4 + i : 5 + i] for i in range(2)]
        out.append((rows, before))
        before = before + (meta[6:7] + meta[7:8] + meta[8:9])
    return out, before


def attend(qa_ref, ka_ref, vt_ref, half, old, new):
    m_out, acc_out = new

    def scores(i, keys):
        start = i * QT if half is not None else pl.multiple_of(i * QT, QT)
        s = lax.dot_general(
            ka_ref[:keys, :],
            qa_ref[pl.ds(start, QT), :],
            (((1,), (1,)), ((), ())),
            preferred_element_type=F32,
        )
        if half is not None:
            row = lax.broadcasted_iota(jnp.int32, (keys, QT), 0)
            col = lax.broadcasted_iota(jnp.int32, (keys, QT), 1)
            pos = row + (row // HALF + half) * HALF
            s = jnp.where(pos <= col + start, s, NEG)
        return s

    def finish(i, keys, s):
        best = jnp.max(s, axis=0, keepdims=True)
        if old is not None:
            before = old[0][i][:1]
            best = jnp.maximum(best, before)
        safe = jnp.where(best < -1e29, 0.0, best)
        w = jnp.exp(s - safe).astype(BF)
        acc = jnp.dot(vt_ref[:, :keys], w, preferred_element_type=F32)
        if old is not None:
            acc = acc + old[1][i] * jnp.exp(before - safe)
        m_out[i] = jnp.broadcast_to(best, (8, QT))
        acc_out[i] = acc

    def run(tiles):
        s = scores(*tiles[0])
        for tile, after in zip(tiles, [*tiles[1:], None]):
            following = scores(*after) if after else None
            finish(*tile, s)
            s = following

    if half is not None:
        run([(i, HALF * (i * QT // BLOCK + 1)) for i in range(TILES)])
    else:
        part = TILES // 2

        def some(j, carry):
            run([(j * part + i, KEYS) for i in range(part)])
            return carry

        lax.fori_loop(0, 2, some, 0)


def whole(ref):
    return [(ref, xs) for xs in range(NX)]


def diag_kernel(ids_ref, q0, q1, q2, q3, kv_ref, qa_out, off_out, m_out, acc_out, ka_ref, vt_ref):
    offsets, _ = slab_offsets(whole(kv_ref))
    fill(whole(kv_ref), offsets, ka_ref, vt_ref)
    lane = lax.broadcasted_iota(jnp.int32, (SLAB, 128), 1)
    for step, q_ref in enumerate((q0, q1, q2, q3)):
        block = (ids_ref[1] + NX - step) % NX
        qa_out[pl.ds(pl.multiple_of(block * BLOCK, BLOCK), BLOCK), :128] = q_ref[...]
    qa_out[:, 128:] = jnp.where(lane < 24, 1.0, 0.0).astype(BF)
    attend(qa_out, ka_ref, vt_ref, ids_ref[1] // 2, None, (m_out, acc_out))
    off_out[...] = jnp.zeros((8, 128), F32)


def shifted(offsets, base):
    return [(rows, before + base) for rows, before in offsets]


def front_kernel(
    step, ids_ref, qa_ref, kv_ref, off_in, m_in, acc_in, off_out, m_out, acc_out, ka_ref, vt_ref
):
    valid = ids_ref[0] >= step

    @pl.when(valid)
    def _():
        offsets, total = slab_offsets(whole(kv_ref))
        base = off_in[:1, :] - total
        fill(whole(kv_ref), shifted(offsets, base), ka_ref, vt_ref)
        attend(qa_ref, ka_ref, vt_ref, None, (m_in, acc_in), (m_out, acc_out))
        off_out[...] = jnp.broadcast_to(base, (8, 128))

    @pl.when(jnp.logical_not(valid))
    def _():
        off_out[...] = off_in[...]
        m_out[...] = m_in[...]
        acc_out[...] = acc_in[...]


def back_kernel(step, ids_ref, qa_ref, kv_ref, *refs):
    ins, (off_out, m_out, acc_out, ka_ref, vt_ref) = refs[:-5], refs[-5:]
    valid = ids_ref[0] + step >= NZ

    @pl.when(valid)
    def _():
        offsets, total = slab_offsets(whole(kv_ref))
        base = ins[0][:1, :] if ins else jnp.zeros((1, 128), F32)
        fill(whole(kv_ref), shifted(offsets, base), ka_ref, vt_ref)
        old = (ins[1], ins[2]) if ins else None
        attend(qa_ref, ka_ref, vt_ref, None, old, (m_out, acc_out))
        off_out[...] = jnp.broadcast_to(base + total, (8, 128))

    @pl.when(jnp.logical_not(valid))
    def _():
        if ins:
            off_out[...] = ins[0][...]
            m_out[...] = ins[1][...]
            acc_out[...] = ins[2][...]
        else:
            off_out[...] = jnp.zeros((8, 128), F32)
            m_out[...] = jnp.full(m_out.shape, NEG, F32)
            acc_out[...] = jnp.zeros(acc_out.shape, F32)


def last_kernel(
    ids_ref, qa_ref, kv0_ref, kv1_ref, foff, fm, facc, boff, bm, bacc, out0, out1, out2, out3,
    off_s, m_s, acc_s, ka_ref, vt_ref,
):
    valid = ids_ref[0] >= 4
    blocks = [(kv0_ref, 0), (kv0_ref, 1), (kv1_ref, 0), (kv1_ref, 1)]

    @pl.when(valid)
    def _():
        offsets, total = slab_offsets(blocks)
        base = foff[:1, :] - total
        fill(blocks, shifted(offsets, base), ka_ref, vt_ref)
        attend(qa_ref, ka_ref, vt_ref, None, (fm, facc), (m_s, acc_s))
        off_s[...] = jnp.broadcast_to(base, (8, 128))

    @pl.when(jnp.logical_not(valid))
    def _():
        off_s[...] = foff[...]
        m_s[...] = fm[...]
        acc_s[...] = facc[...]

    shift = (boff[:1, :] - off_s[:1, :])[:, :1]
    per = BLOCK // QT
    for step, out_ref in enumerate((out0, out1, out2, out3)):
        block = (ids_ref[1] + step) % NX
        stats = []
        for t in range(per):
            stats += merge(block * per + t, t, shift, (m_s, acc_s), (bm, bacc), out_ref)
        part = jnp.concatenate(stats, axis=0)
        rows = jnp.concatenate([*thirds(part), jnp.zeros((META - 12, 128), F32)], axis=0)
        out_ref[BLOCK:, :] = rows.astype(BF)


def merge(i, t, shift, front, back, out_ref):
    (m_s, acc_s), (bm, bacc) = front, back
    best_f = m_s[i, :1, :]
    best_b = jnp.where(bacc[i, 128:129, :] > 0.0, bm[i, :1, :] + shift, NEG)
    best = jnp.maximum(best_f, best_b)
    safe = jnp.where(best < -1e29, 0.0, best)
    wf = jnp.exp(best_f - safe)
    wb = jnp.exp(best_b - safe)
    total = wf * acc_s[i, 128:129, :] + wb * bacc[i, 128:129, :]
    some = total > 0.0
    total = jnp.where(some, total, 1.0)
    wf = wf / total
    wb = wb / total
    mix = wf * acc_s[i, :128, :] + wb * bacc[i, :128, :]
    lse = jnp.where(some, best + jnp.log(total), NEG)
    stats = []
    for g in range(QT // 128):
        row = t * QT + g * 128
        out_ref[row : row + 128, :] = mix[:, g * 128 : (g + 1) * 128].T.astype(BF)
        stats.append(lse[:, g * 128 : (g + 1) * 128])
    return stats


def join_kernel(ids_ref, p0_ref, p1_ref, p2_ref, p3_ref, gate_ref, out_ref):
    shares = []
    for one, two in ((p0_ref, p2_ref), (p1_ref, p3_ref)):
        metas = [ref[BLOCK:, :].astype(F32) for ref in (one, two)]
        first, second = [meta[0:4] + meta[4:8] + meta[8:12] for meta in metas]
        shares.append(1.0 / (1.0 + jnp.exp(second - first)))
    even = ids_ref[1] % 2 == 0
    for g in range(4):
        rows = slice(g * 128, (g + 1) * 128)
        atts = []
        for a, (one, two) in enumerate(((p0_ref, p2_ref), (p1_ref, p3_ref))):
            w0 = jnp.broadcast_to(shares[a][g : g + 1], (128, 128)).T
            mix = w0 * one[rows, :].astype(F32) + (1.0 - w0) * two[rows, :].astype(F32)
            atts.append(mix * gate_ref[a, rows, :])
        low = jnp.where(even, atts[0], atts[1]).astype(BF)
        high = jnp.where(even, atts[1], atts[0]).astype(BF)
        for h in range(2):
            part = slice(h * PIECE, (h + 1) * PIECE)
            out_ref[2 * g + h, :, :128] = low[part]
            out_ref[2 * g + h, :, 128:] = high[part]


def out_kernel(rows_ref, wo_ref, out_ref, lhs_ref):
    for j in range(NY * NC):
        lhs_ref[:, j * COLS : (j + 1) * COLS] = rows_ref[j]
    out_ref[...] = jnp.dot(lhs_ref[...], wo_ref[...], preferred_element_type=F32).astype(BF)


def shape(*dims, dtype=BF):
    return jax.ShapeDtypeStruct(dims, dtype)


def call(kernel, outs, specs, flops, scratch=(), alias=None, mib=16, exps=0):
    return pl.pallas_call(
        kernel,
        out_shape=outs,
        in_specs=specs,
        out_specs=jax.tree.map(lambda _: vspec(), outs),
        scratch_shapes=scratch,
        input_output_aliases=alias or {},
        cost_estimate=pl.CostEstimate(
            flops=flops, bytes_accessed=2 << 20, transcendentals=exps
        ),
        compiler_params=pltpu.CompilerParams(vmem_limit_bytes=mib << 20),
    )


STATE = (
    shape(8, 128, dtype=F32),
    shape(TILES, 8, QT, dtype=F32),
    shape(TILES, ACC, QT, dtype=F32),
)
LOADED = [VMEM((KEYS, 256), BF), VMEM((ACC, KEYS), BF)]


def attention(kernel, outs, n_in, alias=None, scratch=()):
    specs = [sspec()] + [vspec()] * (n_in - 1)
    flops = 4 * SLAB * KEYS * 128
    return call(kernel, outs, specs, flops, [*scratch, *LOADED], alias, 28, SLAB * KEYS)


def ring(size, step):
    return [(i, (i + step) % size) for i in range(size)]


def body(tokens, wq, wk, wv, wg, fw, fbias, wo):
    ids = jnp.stack([lax.axis_index(a) for a in AXES]).astype(jnp.int32)

    near = [tokens] + [lax.ppermute(tokens, "y", ring(NY, s)) for s in (1, 2, 3)]
    far = [lax.ppermute(near[0], "c", ring(NC, 1))]
    far += [lax.ppermute(t, "c", ring(NC, 1)) for t in near[1:]]
    flops = 2 * BLOCK * WIDTH * COLS
    hbm = pl.BlockSpec(memory_space=pltpu.HBM)
    weight = VMEM((WIDTH, COLS), BF)

    def project(kernel, outs, weights, extra=(), specs=(), scratch=()):
        return call(
            kernel, outs, [sspec()] + [hbm] * (8 + len(weights)) + list(specs),
            flops * len(weights),
            [VMEM((BLOCK, WIDTH), BF), *[weight] * len(weights), pltpu.SemaphoreType.DMA((16,))]
            + list(scratch),
            mib=60,
        )(ids, *near, *far, *weights, *extra)

    kvx = project(
        kv_kernel, shape(NX, ROWS, 128), (wk, wv), (fw.T, fbias),
        (vspec(), sspec()), (VMEM((3, 16, BLOCK), F32),),
    )
    kv = lax.all_to_all(kvx, "x", 0, 0, tiled=True)
    same, other = project(query_kernel, (shape(BLOCK, 128),) * 2, (wq,))

    def swap(values):
        out = [values[0]]
        for s in range(1, NX):
            out.append(lax.ppermute(values[s], "x", ring(NX, s)))
        return out

    qs = swap((same, other, same, other))
    gate = project(gate_kernel, shape(2, BLOCK, 128, dtype=F32), (wg,))

    def hop(value, direction):
        return lax.ppermute(value, "z", ring(NZ, direction))

    kf, kb = [kv], [kv]
    for _ in range(1, 4):
        kf.append(hop(kf[-1], 1))
        kb.append(hop(kb[-1], -1))
    far0 = hop(kf[3][:2], 1)
    far1 = hop(kb[3][2:], -1)

    qa, *front = attention(diag_kernel, (shape(SLAB, 256), *STATE), 6)(ids, *qs, kv)
    back = []
    for s in range(1, 4):
        back = attention(
            functools.partial(back_kernel, s), STATE, 3 + len(back),
            {3: 0, 4: 1, 5: 2} if back else None,
        )(ids, qa, kb[s], *back)
        front = attention(
            functools.partial(front_kernel, s), STATE, 6, {3: 0, 4: 1, 5: 2}
        )(ids, qa, kf[s], *front)
    outs = attention(
        last_kernel, (shape(BLOCK + META, 128),) * NX, 10, None, [VMEM(s.shape, F32) for s in STATE]
    )(ids, qa, far0, far1, *front, *back)
    parts = swap(outs)
    att = call(
        join_kernel, shape(NY * NC, PIECE, COLS), [sspec()] + [vspec()] * 5, 1 << 20
    )(ids, *parts, gate)
    rows = lax.all_to_all(att, ("y", "c"), 0, 0, tiled=True)
    return call(
        out_kernel, shape(PIECE, WIDTH), [vspec()] * 2, 2 * PIECE * WIDTH * WIDTH,
        [VMEM((PIECE, WIDTH), BF)],
    )(rows, wo)


AXES = ("z", "x", "y", "c")


def solution(mesh):
    grid = Mesh(mesh.devices.reshape(NZ, NX, NY, NC), AXES)
    cols = P(None, ("y", "c"))

    return jax.shard_map(
        body,
        mesh=grid,
        in_specs=(P(AXES, None), cols, cols, cols, cols, P(), P(), P()),
        out_specs=P(AXES, None),
        check_vma=False,
    )
```

```python
import functools

import jax
import jax.numpy as jnp
from jax import lax
from jax.experimental import pallas as pl
from jax.experimental.pallas import tpu as pltpu
from jax.sharding import Mesh
from jax.sharding import PartitionSpec as P


HEAD_DIM = 128
NZ, NX, NY, NC = 8, 4, 4, 2
BLOCK = 512
HALF = 256
SLAB = NX * BLOCK
PIECE = 64
WIDTH = 2048
COLS = 256
META = 16
ROWS = 2 * HALF + META
NEG = -1e30

VMEM = pltpu.VMEM
SMEM = pltpu.SMEM
BF = jnp.bfloat16
F32 = jnp.float32


def vspec():
    return pl.BlockSpec(memory_space=VMEM)


def sspec():
    return pl.BlockSpec(memory_space=SMEM)


def thirds(value):
    high = value.astype(BF).astype(F32)
    rest = value - high
    mid = rest.astype(BF).astype(F32)
    low = (rest - mid).astype(BF).astype(F32)
    return high, mid, low


def fetch(ids_ref, pieces, toks_ref, weights, sems):
    y, c = ids_ref[2], ids_ref[3]
    pairs = []
    for i in range(8):
        pos = 2 * ((y + NY - i % NY) % NY) + (c if i < NY else 1 - c)
        start = pl.multiple_of(pos * PIECE, PIECE)
        pairs.append((pieces[i], toks_ref.at[pl.ds(start, PIECE), :]))
    parts = 4
    for source, target in weights:
        for i in range(parts):
            rows = pl.ds(i * WIDTH // parts, WIDTH // parts)
            pairs.append((source.at[rows, :], target.at[rows, :]))
    copies = [
        pltpu.make_async_copy(source, target, sems.at[i])
        for i, (source, target) in enumerate(pairs)
    ]
    for copy in copies:
        copy.start()
    return copies[:8], copies[8:]


def wait_all(copies):
    for copy in copies:
        copy.wait()


def kv_kernel(ids_ref, *refs):
    wk_hbm, wv_hbm, fw_ref, bias_ref, kv_ref, toks_ref, wk_ref, wv_ref, sems, parts_ref = refs[8:]
    y, c = ids_ref[2], ids_ref[3]
    weights = [(wk_hbm, wk_ref), (wv_hbm, wv_ref)]
    toks_copies, weight_copies = fetch(ids_ref, refs[:8], toks_ref, weights, sems)
    wait_all(toks_copies)
    toks = toks_ref[...]
    logits = lax.dot_general(
        fw_ref[...], toks, (((1,), (1,)), ((), ())), preferred_element_type=F32
    )
    row = lax.broadcasted_iota(jnp.int32, (16, BLOCK), 0)
    for head in range(16):
        logits = logits + jnp.where(row == head, bias_ref[head], 0.0)
    logs = jnp.minimum(logits, 0.0) - jnp.log1p(jnp.exp(-jnp.abs(logits)))
    row = lax.broadcasted_iota(jnp.int32, (BLOCK, BLOCK), 0)
    col = lax.broadcasted_iota(jnp.int32, (BLOCK, BLOCK), 1)
    upper = (row <= col).astype(BF)
    local = sum(
        jnp.dot(part.astype(BF), upper, preferred_element_type=F32) for part in thirds(logs)
    )
    for i, part in enumerate(thirds(local)):
        parts_ref[i] = part
    wait_all(weight_copies)
    keys = jnp.dot(toks, wk_ref[...], preferred_element_type=F32).astype(BF)
    values = jnp.dot(toks, wv_ref[...], preferred_element_type=F32)
    for a in range(2):
        head = 2 * (2 * y + c) + a
        mine = [parts_ref[i, pl.ds(head, 1), :] for i in range(3)]
        for b in range(2):
            dest = 2 * b + a
            rows = [
                part[:, b * HALF + i * 128 : b * HALF + (i + 1) * 128]
                for part in mine
                for i in range(2)
            ]
            rows += [jnp.broadcast_to(part[:, BLOCK - 1 :], (1, 128)) for part in mine]
            rows.append(jnp.zeros((META - 9, 128), F32))
            kv_ref[dest, :HALF, :] = keys[b * HALF : (b + 1) * HALF, a * 128 : (a + 1) * 128]
            for g in range(2):
                tile = values[b * HALF + g * 128 : b * HALF + (g + 1) * 128, a * 128 : (a + 1) * 128]
                kv_ref[dest, HALF + g * 128 : HALF + (g + 1) * 128, :] = tile.T.astype(BF)
            kv_ref[dest, 2 * HALF :, :] = jnp.concatenate(rows, axis=0).astype(BF)


def by_parity(ids_ref, both):
    even = ids_ref[1] % 2 == 0
    low, high = both[:, :128], both[:, 128:]
    return jnp.where(even, low, high), jnp.where(even, high, low)


def query_kernel(ids_ref, *refs):
    wq_hbm, same_ref, other_ref, toks_ref, wq_ref, sems = refs[8:]
    toks_copies, weight_copies = fetch(ids_ref, refs[:8], toks_ref, [(wq_hbm, wq_ref)], sems)
    wait_all(toks_copies + weight_copies)
    queries = jnp.dot(toks_ref[...], wq_ref[...], preferred_element_type=F32)
    same, other = by_parity(ids_ref, queries * HEAD_DIM**-0.5)
    same_ref[...] = same.astype(BF)
    other_ref[...] = other.astype(BF)


def gate_kernel(ids_ref, *refs):
    wg_hbm, gate_ref, toks_ref, wg_ref, sems = refs[8:]
    toks_copies, weight_copies = fetch(ids_ref, refs[:8], toks_ref, [(wg_hbm, wg_ref)], sems)
    wait_all(toks_copies + weight_copies)
    pre = jnp.dot(toks_ref[...], wg_ref[...], preferred_element_type=F32)
    gate_ref[0], gate_ref[1] = by_parity(ids_ref, 1.0 / (1.0 + jnp.exp(-pre)))


QT = 512
KEYS = NX * HALF
TILES = SLAB // QT
ACC = 144


def fill(blocks, offsets, ka_ref, vt_ref):
    biases = [rows[g] + before for rows, before in offsets for g in range(2)]
    parts = thirds(-jnp.concatenate(biases, axis=0))
    turned = jnp.concatenate([*parts, jnp.zeros((104, 128), F32)], axis=0).T
    lane = lax.broadcasted_iota(jnp.int32, (128, 128), 1)
    for j, (ref, index) in enumerate(blocks):
        ka_ref[j * HALF : (j + 1) * HALF, :128] = ref[index, :HALF, :]
        for g in range(2):
            cols = slice(j * HALF + g * 128, j * HALF + (g + 1) * 128)
            ka_ref[cols, 128:] = jnp.where(lane % 8 == 2 * j + g, turned, 0.0).astype(BF)
            vt_ref[:128, cols] = ref[index, HALF + g * 128 : HALF + (g + 1) * 128, :]
    row = lax.broadcasted_iota(jnp.int32, (ACC - 128, KEYS), 0)
    vt_ref[128:, :] = jnp.where(row == 0, 1.0, 0.0).astype(BF)


def slab_offsets(blocks):
    out = []
    before = jnp.zeros((1, 128), F32)
    for ref, index in blocks:
        meta = ref[index, 2 * HALF :, :].astype(F32)
        rows = [meta[i : i + 1] + meta[2 + i : 3 + i] + meta[4 + i : 5 + i] for i in range(2)]
        out.append((rows, before))
        before = before + (meta[6:7] + meta[7:8] + meta[8:9])
    return out, before


def attend(qa_ref, ka_ref, vt_ref, half, old, new, d):
    m_out, acc_out = new

    def scores(i, keys):
        s = lax.dot_general(
            ka_ref[:keys, :],
            qa_ref[i * QT : (i + 1) * QT, :],
            (((1,), (1,)), ((), ())),
            preferred_element_type=F32,
        )
        if half is not None:
            row = lax.broadcasted_iota(jnp.int32, (keys, QT), 0)
            col = lax.broadcasted_iota(jnp.int32, (keys, QT), 1)
            pos = row + (row // HALF + half) * HALF
            s = jnp.where(pos <= col + i * QT, s, NEG)
        return s

    def weigh(i, keys, s):
        best = jnp.max(s, axis=0, keepdims=True)
        factor = None
        if old is not None:
            before = old[0][d, i][:1]
            best = jnp.maximum(best, before)
        safe = jnp.where(best < -1e29, 0.0, best)
        if old is not None:
            factor = jnp.exp(before - safe)
        m_out[d, i] = jnp.broadcast_to(best, (8, QT))
        return i, keys, jnp.exp(s - safe).astype(BF), factor

    def finish(i, keys, w, factor):
        acc = jnp.dot(vt_ref[:, :keys], w, preferred_element_type=F32)
        if old is not None:
            acc = acc + old[1][d, i] * factor
        acc_out[d, i] = acc

    tiles = [(i, KEYS if half is None else HALF * (i * QT // BLOCK + 1)) for i in range(TILES)]
    s = scores(*tiles[0])
    last = None
    for tile, after in zip(tiles, [*tiles[1:], None]):
        following = scores(*after) if after else None
        if last is not None:
            finish(*last)
        last = weigh(*tile, s)
        s = following
    finish(*last)


def whole(ref):
    return [(ref, xs) for xs in range(NX)]


def diag_kernel(ids_ref, q0, q1, q2, q3, kv_ref, qa_out, off_out, m_out, acc_out, ka_ref, vt_ref):
    offsets, _ = slab_offsets(whole(kv_ref))
    fill(whole(kv_ref), offsets, ka_ref, vt_ref)
    lane = lax.broadcasted_iota(jnp.int32, (SLAB, 128), 1)
    for step, q_ref in enumerate((q0, q1, q2, q3)):
        block = (ids_ref[1] + NX - step) % NX
        qa_out[pl.ds(pl.multiple_of(block * BLOCK, BLOCK), BLOCK), :128] = q_ref[...]
    qa_out[:, 128:] = jnp.where(lane < 24, 1.0, 0.0).astype(BF)
    attend(qa_out, ka_ref, vt_ref, ids_ref[1] // 2, None, (m_out, acc_out), FRONT)
    off_out[...] = jnp.zeros(off_out.shape, F32)
    m_out[BACK] = jnp.full(m_out.shape[1:], NEG, F32)
    acc_out[BACK] = jnp.zeros(acc_out.shape[1:], F32)


def shifted(offsets, base):
    return [(rows, before + base) for rows, before in offsets]


BACK, FRONT = 0, 1


def step_kernel(
    step, ids_ref, qa_ref, back_ref, front_ref, off_in, m_in, acc_in, off_out, m_out, acc_out,
    ka_ref, vt_ref,
):
    z = ids_ref[0]

    def one(d, carry):
        valid = jnp.where(d == BACK, z + step >= NZ, z >= step)

        @pl.when(valid)
        def _():
            @pl.when(d == BACK)
            def _():
                offsets, total = slab_offsets(whole(back_ref))
                base = off_in[BACK, :1, :]
                fill(whole(back_ref), shifted(offsets, base), ka_ref, vt_ref)
                off_out[BACK] = jnp.broadcast_to(base + total, (8, 128))

            @pl.when(d == FRONT)
            def _():
                offsets, total = slab_offsets(whole(front_ref))
                base = off_in[FRONT, :1, :] - total
                fill(whole(front_ref), shifted(offsets, base), ka_ref, vt_ref)
                off_out[FRONT] = jnp.broadcast_to(base, (8, 128))

            attend(qa_ref, ka_ref, vt_ref, None, (m_in, acc_in), (m_out, acc_out), d)

        @pl.when(jnp.logical_not(valid))
        def _():
            off_out[d] = off_in[d]
            m_out[d] = m_in[d]
            acc_out[d] = acc_in[d]

        return carry

    lax.fori_loop(0, 2, one, 0)


def last_kernel(
    ids_ref, qa_ref, kv0_ref, kv1_ref, off_in, m_in, acc_in, out0, out1, out2, out3,
    off_s, m_s, acc_s, ka_ref, vt_ref,
):
    valid = ids_ref[0] >= 4
    blocks = [(kv0_ref, 0), (kv0_ref, 1), (kv1_ref, 0), (kv1_ref, 1)]

    @pl.when(valid)
    def _():
        offsets, total = slab_offsets(blocks)
        base = off_in[FRONT, :1, :] - total
        fill(blocks, shifted(offsets, base), ka_ref, vt_ref)
        attend(qa_ref, ka_ref, vt_ref, None, (m_in, acc_in), (m_s, acc_s), FRONT)
        off_s[...] = jnp.broadcast_to(base, (8, 128))

    @pl.when(jnp.logical_not(valid))
    def _():
        off_s[...] = off_in[FRONT]
        m_s[FRONT] = m_in[FRONT]
        acc_s[FRONT] = acc_in[FRONT]

    shift = (off_in[BACK, :1, :] - off_s[:1, :])[:, :1]
    per = BLOCK // QT
    for step, out_ref in enumerate((out0, out1, out2, out3)):
        block = (ids_ref[1] + step) % NX
        stats = []
        for t in range(per):
            stats += merge(block * per + t, t, shift, (m_s, acc_s), (m_in, acc_in), out_ref)
        part = jnp.concatenate(stats, axis=0)
        rows = jnp.concatenate([*thirds(part), jnp.zeros((META - 12, 128), F32)], axis=0)
        out_ref[BLOCK:, :] = rows.astype(BF)


def merge(i, t, shift, front, back, out_ref):
    (m_s, acc_s), (bm, bacc) = front, back
    best_f = m_s[FRONT, i, :1, :]
    best_b = jnp.where(bacc[BACK, i, 128:129, :] > 0.0, bm[BACK, i, :1, :] + shift, NEG)
    best = jnp.maximum(best_f, best_b)
    safe = jnp.where(best < -1e29, 0.0, best)
    wf = jnp.exp(best_f - safe)
    wb = jnp.exp(best_b - safe)
    total = wf * acc_s[FRONT, i, 128:129, :] + wb * bacc[BACK, i, 128:129, :]
    some = total > 0.0
    total = jnp.where(some, total, 1.0)
    wf = wf / total
    wb = wb / total
    mix = wf * acc_s[FRONT, i, :128, :] + wb * bacc[BACK, i, :128, :]
    lse = jnp.where(some, best + jnp.log(total), NEG)
    stats = []
    for g in range(QT // 128):
        row = t * QT + g * 128
        out_ref[row : row + 128, :] = mix[:, g * 128 : (g + 1) * 128].T.astype(BF)
        stats.append(lse[:, g * 128 : (g + 1) * 128])
    return stats


def join_kernel(ids_ref, p0_ref, p1_ref, p2_ref, p3_ref, gate_ref, out_ref):
    shares = []
    for one, two in ((p0_ref, p2_ref), (p1_ref, p3_ref)):
        metas = [ref[BLOCK:, :].astype(F32) for ref in (one, two)]
        first, second = [meta[0:4] + meta[4:8] + meta[8:12] for meta in metas]
        shares.append(1.0 / (1.0 + jnp.exp(second - first)))
    even = ids_ref[1] % 2 == 0
    for g in range(4):
        rows = slice(g * 128, (g + 1) * 128)
        atts = []
        for a, (one, two) in enumerate(((p0_ref, p2_ref), (p1_ref, p3_ref))):
            w0 = jnp.broadcast_to(shares[a][g : g + 1], (128, 128)).T
            mix = w0 * one[rows, :].astype(F32) + (1.0 - w0) * two[rows, :].astype(F32)
            atts.append(mix * gate_ref[a, rows, :])
        low = jnp.where(even, atts[0], atts[1]).astype(BF)
        high = jnp.where(even, atts[1], atts[0]).astype(BF)
        for h in range(2):
            part = slice(h * PIECE, (h + 1) * PIECE)
            out_ref[2 * g + h, :, :128] = low[part]
            out_ref[2 * g + h, :, 128:] = high[part]


def out_kernel(rows_ref, wo_ref, out_ref, lhs_ref):
    for j in range(NY * NC):
        lhs_ref[:, j * COLS : (j + 1) * COLS] = rows_ref[j]
    out_ref[...] = jnp.dot(lhs_ref[...], wo_ref[...], preferred_element_type=F32).astype(BF)


def shape(*dims, dtype=BF):
    return jax.ShapeDtypeStruct(dims, dtype)


def call(kernel, outs, specs, flops, scratch=(), alias=None, mib=16, exps=0):
    return pl.pallas_call(
        kernel,
        out_shape=outs,
        in_specs=specs,
        out_specs=jax.tree.map(lambda _: vspec(), outs),
        scratch_shapes=scratch,
        input_output_aliases=alias or {},
        cost_estimate=pl.CostEstimate(
            flops=flops, bytes_accessed=2 << 20, transcendentals=exps
        ),
        compiler_params=pltpu.CompilerParams(vmem_limit_bytes=mib << 20),
    )


STATE = (
    shape(2, 8, 128, dtype=F32),
    shape(2, TILES, 8, QT, dtype=F32),
    shape(2, TILES, ACC, QT, dtype=F32),
)
LOADED = [VMEM((KEYS, 256), BF), VMEM((ACC, KEYS), BF)]


def attention(kernel, outs, n_in, alias=None, scratch=()):
    specs = [sspec()] + [vspec()] * (n_in - 1)
    flops = 4 * SLAB * KEYS * 128
    return call(kernel, outs, specs, flops, [*scratch, *LOADED], alias, 28, SLAB * KEYS)


def ring(size, step):
    return [(i, (i + step) % size) for i in range(size)]


def body(tokens, wq, wk, wv, wg, fw, fbias, wo):
    ids = jnp.stack([lax.axis_index(a) for a in AXES]).astype(jnp.int32)

    near = [tokens] + [lax.ppermute(tokens, "y", ring(NY, s)) for s in (1, 2, 3)]
    far = [lax.ppermute(near[0], "c", ring(NC, 1))]
    far += [lax.ppermute(t, "c", ring(NC, 1)) for t in near[1:]]
    flops = 2 * BLOCK * WIDTH * COLS
    hbm = pl.BlockSpec(memory_space=pltpu.HBM)
    weight = VMEM((WIDTH, COLS), BF)

    def project(kernel, outs, weights, extra=(), specs=(), scratch=()):
        return call(
            kernel, outs, [sspec()] + [hbm] * (8 + len(weights)) + list(specs),
            flops * len(weights),
            [VMEM((BLOCK, WIDTH), BF), *[weight] * len(weights), pltpu.SemaphoreType.DMA((16,))]
            + list(scratch),
            mib=60,
        )(ids, *near, *far, *weights, *extra)

    kvx = project(
        kv_kernel, shape(NX, ROWS, 128), (wk, wv), (fw.T, fbias),
        (vspec(), sspec()), (VMEM((3, 16, BLOCK), F32),),
    )
    kv = lax.all_to_all(kvx, "x", 0, 0, tiled=True)
    same, other = project(query_kernel, (shape(BLOCK, 128),) * 2, (wq,))

    def swap(values):
        out = [values[0]]
        for s in range(1, NX):
            out.append(lax.ppermute(values[s], "x", ring(NX, s)))
        return out

    qs = swap((same, other, same, other))
    gate = project(gate_kernel, shape(2, BLOCK, 128, dtype=F32), (wg,))

    def hop(value, direction):
        return lax.ppermute(value, "z", ring(NZ, direction))

    kf, kb = [kv], [kv]
    for _ in range(1, 4):
        kf.append(hop(kf[-1], 1))
        kb.append(hop(kb[-1], -1))
    far0 = hop(kf[3][:2], 1)
    far1 = hop(kb[3][2:], -1)

    qa, *state = attention(diag_kernel, (shape(SLAB, 256), *STATE), 6)(ids, *qs, kv)
    for s in range(1, 4):
        state = attention(
            functools.partial(step_kernel, s), STATE, 7, {4: 0, 5: 1, 6: 2}
        )(ids, qa, kb[s], kf[s], *state)
    outs = attention(
        last_kernel,
        (shape(BLOCK + META, 128),) * NX,
        7,
        None,
        [VMEM((8, 128), F32), *(VMEM(s.shape, F32) for s in STATE[1:])],
    )(ids, qa, far0, far1, *state)
    parts = swap(outs)
    att = call(join_kernel, shape(NY * NC, PIECE, COLS), [sspec()] + [vspec()] * 5, 1 << 20)(ids, *parts, gate)
    rows = lax.all_to_all(att, ("y", "c"), 0, 0, tiled=True)
    return call(
        out_kernel, shape(PIECE, WIDTH), [vspec()] * 2, 2 * PIECE * WIDTH * WIDTH,
        [VMEM((PIECE, WIDTH), BF)],
    )(rows, wo)


AXES = ("z", "x", "y", "c")


def solution(mesh):
    grid = Mesh(mesh.devices.reshape(NZ, NX, NY, NC), AXES)
    cols = P(None, ("y", "c"))

    return jax.shard_map(
        body,
        mesh=grid,
        in_specs=(P(AXES, None), cols, cols, cols, cols, P(), P(), P()),
        out_specs=P(AXES, None),
        check_vma=False,
    )
```

```python
import functools

import jax
import jax.numpy as jnp
from jax import lax
from jax.experimental import pallas as pl
from jax.experimental.pallas import tpu as pltpu
from jax.sharding import Mesh
from jax.sharding import PartitionSpec as P


HEAD_DIM = 128
NZ, NX, NY, NC = 8, 4, 4, 2
BLOCK = 512
HALF = 256
SLAB = NX * BLOCK
PIECE = 64
PIECES = 10
WIDTH = 2048
COLS = 256
META = 16
ROWS = 2 * HALF + META
NEG = -1e30

VMEM = pltpu.VMEM
SMEM = pltpu.SMEM
BF = jnp.bfloat16
F32 = jnp.float32


def vspec():
    return pl.BlockSpec(memory_space=VMEM)


def sspec():
    return pl.BlockSpec(memory_space=SMEM)


def thirds(value):
    high = value.astype(BF).astype(F32)
    rest = value - high
    mid = rest.astype(BF).astype(F32)
    low = (rest - mid).astype(BF).astype(F32)
    return high, mid, low


def fetch(ids_ref, pieces, toks_ref, weights, sems):
    y, c = ids_ref[2], ids_ref[3]
    pairs = []
    for i, piece in enumerate(pieces):
        away, offset = ((0, 0), (1, 0), (3, 0), (2, 0), (2, PIECE // 2))[i % 5]
        pos = 2 * ((y + NY - away) % NY) + (c if i < 5 else 1 - c)
        start = pl.multiple_of(pos * PIECE + offset, PIECE // 2)
        pairs.append((piece, toks_ref.at[pl.ds(start, piece.shape[0]), :]))
    parts = 4
    for source, target in weights:
        for i in range(parts):
            rows = pl.ds(i * WIDTH // parts, WIDTH // parts)
            pairs.append((source.at[rows, :], target.at[rows, :]))
    copies = [
        pltpu.make_async_copy(source, target, sems.at[i])
        for i, (source, target) in enumerate(pairs)
    ]
    for copy in copies:
        copy.start()
    return copies[: len(pieces)], copies[len(pieces) :]


def wait_all(copies):
    for copy in copies:
        copy.wait()


def kv_kernel(ids_ref, *refs):
    wk_hbm, wv_hbm, fw_ref, bias_ref, kv_ref, toks_ref, wk_ref, wv_ref, sems, parts_ref = refs[PIECES:]
    y, c = ids_ref[2], ids_ref[3]
    weights = [(wk_hbm, wk_ref), (wv_hbm, wv_ref)]
    toks_copies, weight_copies = fetch(ids_ref, refs[:PIECES], toks_ref, weights, sems)
    wait_all(toks_copies)
    toks = toks_ref[...]
    logits = lax.dot_general(
        fw_ref[...], toks, (((1,), (1,)), ((), ())), preferred_element_type=F32
    )
    row = lax.broadcasted_iota(jnp.int32, (16, BLOCK), 0)
    for head in range(16):
        logits = logits + jnp.where(row == head, bias_ref[head], 0.0)
    logs = jnp.minimum(logits, 0.0) - jnp.log1p(jnp.exp(-jnp.abs(logits)))
    row = lax.broadcasted_iota(jnp.int32, (BLOCK, BLOCK), 0)
    col = lax.broadcasted_iota(jnp.int32, (BLOCK, BLOCK), 1)
    upper = (row <= col).astype(BF)
    local = sum(
        jnp.dot(part.astype(BF), upper, preferred_element_type=F32) for part in thirds(logs)
    )
    for i, part in enumerate(thirds(local)):
        parts_ref[i] = part
    wait_all(weight_copies)
    keys = jnp.dot(toks, wk_ref[...], preferred_element_type=F32).astype(BF)
    values = jnp.dot(toks, wv_ref[...], preferred_element_type=F32)
    for a in range(2):
        head = 2 * (2 * y + c) + a
        mine = [parts_ref[i, pl.ds(head, 1), :] for i in range(3)]
        for b in range(2):
            dest = 2 * b + a
            rows = [
                part[:, b * HALF + i * 128 : b * HALF + (i + 1) * 128]
                for part in mine
                for i in range(2)
            ]
            rows += [jnp.broadcast_to(part[:, BLOCK - 1 :], (1, 128)) for part in mine]
            rows.append(jnp.zeros((META - 9, 128), F32))
            kv_ref[dest, :HALF, :] = keys[b * HALF : (b + 1) * HALF, a * 128 : (a + 1) * 128]
            for g in range(2):
                tile = values[b * HALF + g * 128 : b * HALF + (g + 1) * 128, a * 128 : (a + 1) * 128]
                kv_ref[dest, HALF + g * 128 : HALF + (g + 1) * 128, :] = tile.T.astype(BF)
            kv_ref[dest, 2 * HALF :, :] = jnp.concatenate(rows, axis=0).astype(BF)


def by_parity(ids_ref, both):
    even = ids_ref[1] % 2 == 0
    low, high = both[:, :128], both[:, 128:]
    return jnp.where(even, low, high), jnp.where(even, high, low)


def query_kernel(ids_ref, *refs):
    wq_hbm, same_ref, other_ref, toks_ref, wq_ref, sems = refs[PIECES:]
    toks_copies, weight_copies = fetch(ids_ref, refs[:PIECES], toks_ref, [(wq_hbm, wq_ref)], sems)
    wait_all(toks_copies + weight_copies)
    queries = jnp.dot(toks_ref[...], wq_ref[...], preferred_element_type=F32)
    same, other = by_parity(ids_ref, queries * HEAD_DIM**-0.5)
    same_ref[...] = same.astype(BF)
    other_ref[...] = other.astype(BF)


def gate_kernel(ids_ref, *refs):
    wg_hbm, gate_ref, toks_ref, wg_ref, sems = refs[PIECES:]
    toks_copies, weight_copies = fetch(ids_ref, refs[:PIECES], toks_ref, [(wg_hbm, wg_ref)], sems)
    wait_all(toks_copies + weight_copies)
    pre = jnp.dot(toks_ref[...], wg_ref[...], preferred_element_type=F32)
    gate_ref[0], gate_ref[1] = by_parity(ids_ref, 1.0 / (1.0 + jnp.exp(-pre)))


QT = 512
KEYS = NX * HALF
TILES = SLAB // QT
ACC = 144


def fill(blocks, offsets, ka_ref, vt_ref):
    biases = [rows[g] + before for rows, before in offsets for g in range(2)]
    parts = thirds(-jnp.concatenate(biases, axis=0))
    turned = jnp.concatenate([*parts, jnp.zeros((104, 128), F32)], axis=0).T
    lane = lax.broadcasted_iota(jnp.int32, (128, 128), 1)
    for j, (ref, index) in enumerate(blocks):
        ka_ref[j * HALF : (j + 1) * HALF, :128] = ref[index, :HALF, :]
        for g in range(2):
            cols = slice(j * HALF + g * 128, j * HALF + (g + 1) * 128)
            ka_ref[cols, 128:] = jnp.where(lane % 8 == 2 * j + g, turned, 0.0).astype(BF)
            vt_ref[:128, cols] = ref[index, HALF + g * 128 : HALF + (g + 1) * 128, :]
    row = lax.broadcasted_iota(jnp.int32, (ACC - 128, KEYS), 0)
    vt_ref[128:, :] = jnp.where(row == 0, 1.0, 0.0).astype(BF)


def slab_offsets(blocks):
    out = []
    before = jnp.zeros((1, 128), F32)
    for ref, index in blocks:
        meta = ref[index, 2 * HALF :, :].astype(F32)
        rows = [meta[i : i + 1] + meta[2 + i : 3 + i] + meta[4 + i : 5 + i] for i in range(2)]
        out.append((rows, before))
        before = before + (meta[6:7] + meta[7:8] + meta[8:9])
    return out, before


def attend(qa_ref, ka_ref, vt_ref, half, old, new, d):
    m_out, acc_out = new

    def scores(i, keys):
        s = lax.dot_general(
            ka_ref[:keys, :],
            qa_ref[i * QT : (i + 1) * QT, :],
            (((1,), (1,)), ((), ())),
            preferred_element_type=F32,
        )
        if half is not None:
            row = lax.broadcasted_iota(jnp.int32, (keys, QT), 0)
            col = lax.broadcasted_iota(jnp.int32, (keys, QT), 1)
            pos = row + (row // HALF + half) * HALF
            s = jnp.where(pos <= col + i * QT, s, NEG)
        return s

    def weigh(i, keys, s):
        best = jnp.max(s, axis=0, keepdims=True)
        factor = None
        if old is not None:
            before = old[0][d, i][:1]
            best = jnp.maximum(best, before)
        safe = jnp.where(best < -1e29, 0.0, best)
        if old is not None:
            factor = jnp.exp(before - safe)
        m_out[d, i] = jnp.broadcast_to(best, (8, QT))
        return i, keys, jnp.exp(s - safe).astype(BF), factor

    def finish(i, keys, w, factor):
        acc = jnp.dot(vt_ref[:, :keys], w, preferred_element_type=F32)
        if old is not None:
            acc = acc + old[1][d, i] * factor
        acc_out[d, i] = acc

    tiles = [(i, KEYS if half is None else HALF * (i * QT // BLOCK + 1)) for i in range(TILES)]
    s = scores(*tiles[0])
    last = None
    for tile, after in zip(tiles, [*tiles[1:], None]):
        following = scores(*after) if after else None
        if last is not None:
            finish(*last)
        last = weigh(*tile, s)
        s = following
    finish(*last)


def whole(ref):
    return [(ref, xs) for xs in range(NX)]


def diag_kernel(ids_ref, q0, q1, q2, q3, kv_ref, qa_out, off_out, m_out, acc_out, ka_ref, vt_ref):
    offsets, _ = slab_offsets(whole(kv_ref))
    fill(whole(kv_ref), offsets, ka_ref, vt_ref)
    lane = lax.broadcasted_iota(jnp.int32, (SLAB, 128), 1)
    for step, q_ref in enumerate((q0, q1, q2, q3)):
        block = (ids_ref[1] + NX - step) % NX
        qa_out[pl.ds(pl.multiple_of(block * BLOCK, BLOCK), BLOCK), :128] = q_ref[...]
    qa_out[:, 128:] = jnp.where(lane < 24, 1.0, 0.0).astype(BF)
    attend(qa_out, ka_ref, vt_ref, ids_ref[1] // 2, None, (m_out, acc_out), FRONT)
    off_out[...] = jnp.zeros(off_out.shape, F32)
    m_out[BACK] = jnp.full(m_out.shape[1:], NEG, F32)
    acc_out[BACK] = jnp.zeros(acc_out.shape[1:], F32)


def shifted(offsets, base):
    return [(rows, before + base) for rows, before in offsets]


BACK, FRONT = 0, 1


def step_kernel(
    step, ids_ref, qa_ref, back_ref, front_ref, off_in, m_in, acc_in, off_out, m_out, acc_out,
    ka_ref, vt_ref,
):
    z = ids_ref[0]

    def one(d, carry):
        valid = jnp.where(d == BACK, z + step >= NZ, z >= step)

        @pl.when(valid)
        def _():
            @pl.when(d == BACK)
            def _():
                offsets, total = slab_offsets(whole(back_ref))
                base = off_in[BACK, :1, :]
                fill(whole(back_ref), shifted(offsets, base), ka_ref, vt_ref)
                off_out[BACK] = jnp.broadcast_to(base + total, (8, 128))

            @pl.when(d == FRONT)
            def _():
                offsets, total = slab_offsets(whole(front_ref))
                base = off_in[FRONT, :1, :] - total
                fill(whole(front_ref), shifted(offsets, base), ka_ref, vt_ref)
                off_out[FRONT] = jnp.broadcast_to(base, (8, 128))

            attend(qa_ref, ka_ref, vt_ref, None, (m_in, acc_in), (m_out, acc_out), d)

        @pl.when(jnp.logical_not(valid))
        def _():
            off_out[d] = off_in[d]
            m_out[d] = m_in[d]
            acc_out[d] = acc_in[d]

        return carry

    lax.fori_loop(0, 2, one, 0)


def last_kernel(
    ids_ref, qa_ref, kv0_ref, kv1_ref, off_in, m_in, acc_in, out0, out1, out2, out3,
    off_s, m_s, acc_s, ka_ref, vt_ref,
):
    valid = ids_ref[0] >= 4
    blocks = [(kv0_ref, 0), (kv0_ref, 1), (kv1_ref, 0), (kv1_ref, 1)]

    @pl.when(valid)
    def _():
        offsets, total = slab_offsets(blocks)
        base = off_in[FRONT, :1, :] - total
        fill(blocks, shifted(offsets, base), ka_ref, vt_ref)
        attend(qa_ref, ka_ref, vt_ref, None, (m_in, acc_in), (m_s, acc_s), FRONT)
        off_s[...] = jnp.broadcast_to(base, (8, 128))

    @pl.when(jnp.logical_not(valid))
    def _():
        off_s[...] = off_in[FRONT]
        m_s[FRONT] = m_in[FRONT]
        acc_s[FRONT] = acc_in[FRONT]

    shift = (off_in[BACK, :1, :] - off_s[:1, :])[:, :1]
    per = BLOCK // QT
    for step, out_ref in enumerate((out0, out1, out2, out3)):
        block = (ids_ref[1] + step) % NX
        stats = []
        for t in range(per):
            stats += merge(block * per + t, t, shift, (m_s, acc_s), (m_in, acc_in), out_ref)
        part = jnp.concatenate(stats, axis=0)
        rows = jnp.concatenate([*thirds(part), jnp.zeros((META - 12, 128), F32)], axis=0)
        out_ref[BLOCK:, :] = rows.astype(BF)


def merge(i, t, shift, front, back, out_ref):
    (m_s, acc_s), (bm, bacc) = front, back
    best_f = m_s[FRONT, i, :1, :]
    best_b = jnp.where(bacc[BACK, i, 128:129, :] > 0.0, bm[BACK, i, :1, :] + shift, NEG)
    best = jnp.maximum(best_f, best_b)
    safe = jnp.where(best < -1e29, 0.0, best)
    wf = jnp.exp(best_f - safe)
    wb = jnp.exp(best_b - safe)
    total = wf * acc_s[FRONT, i, 128:129, :] + wb * bacc[BACK, i, 128:129, :]
    some = total > 0.0
    total = jnp.where(some, total, 1.0)
    wf = wf / total
    wb = wb / total
    mix = wf * acc_s[FRONT, i, :128, :] + wb * bacc[BACK, i, :128, :]
    lse = jnp.where(some, best + jnp.log(total), NEG)
    stats = []
    for g in range(QT // 128):
        row = t * QT + g * 128
        out_ref[row : row + 128, :] = mix[:, g * 128 : (g + 1) * 128].T.astype(BF)
        stats.append(lse[:, g * 128 : (g + 1) * 128])
    return stats


def join_kernel(ids_ref, p0_ref, p1_ref, p2_ref, p3_ref, gate_ref, out_ref):
    shares = []
    for one, two in ((p0_ref, p2_ref), (p1_ref, p3_ref)):
        metas = [ref[BLOCK:, :].astype(F32) for ref in (one, two)]
        first, second = [meta[0:4] + meta[4:8] + meta[8:12] for meta in metas]
        shares.append(1.0 / (1.0 + jnp.exp(second - first)))
    even = ids_ref[1] % 2 == 0
    for g in range(4):
        rows = slice(g * 128, (g + 1) * 128)
        atts = []
        for a, (one, two) in enumerate(((p0_ref, p2_ref), (p1_ref, p3_ref))):
            w0 = jnp.broadcast_to(shares[a][g : g + 1], (128, 128)).T
            mix = w0 * one[rows, :].astype(F32) + (1.0 - w0) * two[rows, :].astype(F32)
            atts.append(mix * gate_ref[a, rows, :])
        low = jnp.where(even, atts[0], atts[1]).astype(BF)
        high = jnp.where(even, atts[1], atts[0]).astype(BF)
        for h in range(2):
            part = slice(h * PIECE, (h + 1) * PIECE)
            out_ref[2 * g + h, :, :128] = low[part]
            out_ref[2 * g + h, :, 128:] = high[part]


def out_kernel(rows_ref, wo_ref, out_ref, lhs_ref):
    for j in range(NY * NC):
        lhs_ref[:, j * COLS : (j + 1) * COLS] = rows_ref[j]
    out_ref[...] = jnp.dot(lhs_ref[...], wo_ref[...], preferred_element_type=F32).astype(BF)


def shape(*dims, dtype=BF):
    return jax.ShapeDtypeStruct(dims, dtype)


def call(kernel, outs, specs, flops, scratch=(), alias=None, mib=16, exps=0):
    return pl.pallas_call(
        kernel,
        out_shape=outs,
        in_specs=specs,
        out_specs=jax.tree.map(lambda _: vspec(), outs),
        scratch_shapes=scratch,
        input_output_aliases=alias or {},
        cost_estimate=pl.CostEstimate(
            flops=flops, bytes_accessed=2 << 20, transcendentals=exps
        ),
        compiler_params=pltpu.CompilerParams(vmem_limit_bytes=mib << 20),
    )


STATE = (
    shape(2, 8, 128, dtype=F32),
    shape(2, TILES, 8, QT, dtype=F32),
    shape(2, TILES, ACC, QT, dtype=F32),
)
LOADED = [VMEM((KEYS, 256), BF), VMEM((ACC, KEYS), BF)]


def attention(kernel, outs, n_in, alias=None, scratch=()):
    specs = [sspec()] + [vspec()] * (n_in - 1)
    flops = 4 * SLAB * KEYS * 128
    return call(kernel, outs, specs, flops, [*scratch, *LOADED], alias, 28, SLAB * KEYS)


def ring(size, step):
    return [(i, (i + step) % size) for i in range(size)]


def body(tokens, wq, wk, wv, wg, fw, fbias, wo):
    ids = jnp.stack([lax.axis_index(a) for a in AXES]).astype(jnp.int32)

    top = PIECE // 2
    direct = lax.ppermute(tokens[:top], "y", ring(NY, 2))
    left = lax.ppermute(tokens, "y", ring(NY, 1))
    right = lax.ppermute(tokens, "y", ring(NY, 3))
    mate = lax.ppermute(tokens, "c", ring(NC, 1))
    relayed = lax.ppermute(left[top:], "y", ring(NY, 1))
    near = [tokens, left, right, direct, relayed]
    far = [mate] + [lax.ppermute(t, "c", ring(NC, 1)) for t in near[1:]]
    flops = 2 * BLOCK * WIDTH * COLS
    hbm = pl.BlockSpec(memory_space=pltpu.HBM)
    weight = VMEM((WIDTH, COLS), BF)

    def project(kernel, outs, weights, extra=(), specs=(), scratch=()):
        return call(
            kernel, outs, [sspec()] + [hbm] * (PIECES + len(weights)) + list(specs),
            flops * len(weights),
            [VMEM((BLOCK, WIDTH), BF), *[weight] * len(weights), pltpu.SemaphoreType.DMA((18,))]
            + list(scratch),
            mib=60,
        )(ids, *near, *far, *weights, *extra)

    kvx = project(
        kv_kernel, shape(NX, ROWS, 128), (wk, wv), (fw.T, fbias),
        (vspec(), sspec()), (VMEM((3, 16, BLOCK), F32),),
    )
    kv = lax.all_to_all(kvx, "x", 0, 0, tiled=True)
    same, other = project(query_kernel, (shape(BLOCK, 128),) * 2, (wq,))

    def swap(values):
        out = [values[0]]
        for s in range(1, NX):
            out.append(lax.ppermute(values[s], "x", ring(NX, s)))
        return out

    qs = swap((same, other, same, other))
    gate = project(gate_kernel, shape(2, BLOCK, 128, dtype=F32), (wg,))

    def hop(value, direction):
        return lax.ppermute(value, "z", ring(NZ, direction))

    kf, kb = [kv], [kv]
    for _ in range(1, 4):
        kf.append(hop(kf[-1], 1))
        kb.append(hop(kb[-1], -1))
    far0 = hop(kf[3][:2], 1)
    far1 = hop(kb[3][2:], -1)

    qa, *state = attention(diag_kernel, (shape(SLAB, 256), *STATE), 6)(ids, *qs, kv)
    for s in range(1, 4):
        state = attention(
            functools.partial(step_kernel, s), STATE, 7, {4: 0, 5: 1, 6: 2}
        )(ids, qa, kb[s], kf[s], *state)
    outs = attention(
        last_kernel,
        (shape(BLOCK + META, 128),) * NX,
        7,
        None,
        [VMEM((8, 128), F32), *(VMEM(s.shape, F32) for s in STATE[1:])],
    )(ids, qa, far0, far1, *state)
    parts = swap(outs)
    att = call(join_kernel, shape(NY * NC, PIECE, COLS), [sspec()] + [vspec()] * 5, 1 << 20)(ids, *parts, gate)
    rows = lax.all_to_all(att, ("y", "c"), 0, 0, tiled=True)
    return call(
        out_kernel, shape(PIECE, WIDTH), [vspec()] * 2, 2 * PIECE * WIDTH * WIDTH,
        [VMEM((PIECE, WIDTH), BF)],
    )(rows, wo)


AXES = ("z", "x", "y", "c")


def solution(mesh):
    grid = Mesh(mesh.devices.reshape(NZ, NX, NY, NC), AXES)
    cols = P(None, ("y", "c"))

    return jax.shard_map(
        body,
        mesh=grid,
        in_specs=(P(AXES, None), cols, cols, cols, cols, P(), P(), P()),
        out_specs=P(AXES, None),
        check_vma=False,
    )
```
